32 devices in a mesh: sp: 4 (over z), fs: 4 (over y, x), tp: 2 (over core).
Axes of the slice: x: 2, y: 2, z: 4, core: 2. Of those that a mesh axis runs over, the one named last changes fastest.
Arguments:
- tokens: bfloat16 [2048, 2048], P(('fs', 'sp')), parts along dimension 0, may hold values from -6 to 6
- norm_gain: bfloat16 [2048], replicated, may hold values from 0.099609375 to 1.8984375
- query_down: bfloat16 [2048, 512], P('sp'), may hold values from -0.125 to 0.125
- query_gain: bfloat16 [512], replicated, may hold values from 0.099609375 to 1.8984375
- latent_down: bfloat16 [2048, 256], replicated, may hold values from -0.125 to 0.125
- latent_gain: bfloat16 [256], replicated, may hold values from 0.099609375 to 1.8984375
- rope_down: bfloat16 [2048, 64], replicated, may hold values from -30 to 30
- query_up: bfloat16 [512, 1536], P(None, 'tp'), may hold values from -0.25 to 0.25
- key_up: bfloat16 [256, 1024], P(None, 'tp'), may hold values from -0.75 to 0.75
- value_up: bfloat16 [256, 1024], P(None, 'tp'), may hold values from -0.375 to 0.375
- glu_value: bfloat16 [2048, 1024], P('sp', 'tp'), may hold values from -0.125 to 0.125
- glu_gate: bfloat16 [2048, 1024], P('sp', 'tp'), may hold values from -0.125 to 0.125
- conv_taps: bfloat16 [31, 1024], P(None, 'tp'), may hold values from -1 to 1
- group_gain: bfloat16 [1024], P('tp'), may hold values from 0.099609375 to 1.8984375
- head_proj: bfloat16 [1024, 2048], P('tp', 'sp'), may hold values from -0.75 to 0.75
- channel_proj: bfloat16 [1024, 2048], P('tp', 'sp'), may hold values from -0.1875 to 0.1875
Outputs:
- mixed_out: bfloat16 [2048, 2048], P(('fs', 'sp'), 'tp'), parts along dimension 0
- log_weight: float32 [8, 2048], P('tp', ('fs', 'sp')), parts along dimension 1
The draws below stay inside these ranges and needn't reach their ends.
There are 4 independent parts, one for each index of `fs`. The reference program is written for one: setup_inputs(seed, part) draws one part's arguments, and reference() takes and returns one part's arrays. A program takes and returns all parts, laid end to end along the dimension named above; an argument that names none is the same for every part. Nothing has to cross between parts.
All inputs are finite; a program needn't handle non-finite values.
Results may differ from the reference program's by a relative error of at most 0.015.
The reference program's roundings to bfloat16 on the way count: a program that leaves them out, or rounds other values in their place, can miss the bound.
Values may be sent and summed in bfloat16 or wider, within the bound.
A program may use at most 128 MiB of HBM per device.

```python
import jax
import jax.numpy as jnp
from jax import lax

D = 2048
HEADS = 8
NOPE = 128
ROPE = 64
VDIM = 128
QR = 512
KVR = 256
CH = 1024
GROUPS = 8
WIDTH = 31
GRID_W = 64
TOK_DEV = 128
LENGTH = 512
N_TP = 2


def draw_rope_down(key, part):
    base_key = jax.random.fold_in(jax.random.fold_in(key, 11), 0)
    entries = jax.random.normal(base_key, (D, ROPE), jnp.float32) * D ** (-0.5)
    return jnp.clip(entries, -30.0, 30.0).astype(jnp.bfloat16)


def steps_of(key, extent, cuts, least, high):
    factor_of, own = 1.0, jax.random.fold_in(key, 6)
    for position, blocks in cuts:
        steps = jnp.exp(jax.random.uniform(jax.random.fold_in(own, position), (blocks,), jnp.float32, least / len(cuts), high / len(cuts)))
        factor_of = factor_of * jnp.repeat(steps, extent[position] // blocks).reshape([-1 if axis == position else 1 for axis in range(len(extent))])
    return factor_of


def bell_draw(stream_key, extent, width, bound, cuts=(), held_as=jnp.bfloat16):
    loudness = steps_of(stream_key, extent, cuts, -0.22, 0.18) if cuts else 1.0
    drawn = jax.random.normal(stream_key, extent, jnp.float32) * width * loudness
    return jnp.minimum(jnp.maximum(drawn, -bound), bound).astype(held_as)


def setup_inputs(seed: int = 0, part: int = 0) -> dict:
    arg_keys = jax.random.split(jax.random.key(seed), 17)
    part_splits = jax.random.split(jax.random.fold_in(arg_keys[16], part), 17)
    tokens = bell_draw(part_splits[0], (LENGTH, D), 1.0, 6.0, ((0, 4),))
    norm_gain = jnp.clip(1.0 + 0.18 * jax.random.normal(arg_keys[1], (D,), jnp.float32), 0.099609375, 1.8984375).astype(jnp.bfloat16)
    query_down = bell_draw(arg_keys[2], (D, QR), D ** -0.5, 0.125, ((0, 4),))
    query_gain = jnp.clip(1.0 + 0.18 * jax.random.normal(arg_keys[3], (QR,), jnp.float32), 0.099609375, 1.8984375).astype(jnp.bfloat16)
    latent_down = bell_draw(arg_keys[4], (D, KVR), D ** -0.5, 0.125)
    latent_gain = jnp.clip(1.0 + 0.18 * jax.random.normal(arg_keys[5], (KVR,), jnp.float32), 0.099609375, 1.8984375).astype(jnp.bfloat16)
    rope_down = draw_rope_down(jax.random.fold_in(arg_keys[16], 71), part)
    query_up = bell_draw(arg_keys[7], (QR, HEADS * (NOPE + ROPE)), QR ** -0.5, 0.25, ((1, 2),))
    key_up = bell_draw(arg_keys[8], (KVR, HEADS * NOPE), 0.125, 0.75, ((1, 2),))
    value_up = bell_draw(arg_keys[9], (KVR, HEADS * VDIM), KVR ** -0.5, 0.375, ((1, 2),))
    glu_value = bell_draw(arg_keys[10], (D, CH), D ** -0.5, 0.125, ((0, 4), (1, 2)))
    glu_gate = bell_draw(arg_keys[11], (D, CH), D ** -0.5, 0.125, ((0, 4), (1, 2)))
    conv_taps = bell_draw(arg_keys[12], (WIDTH, CH), WIDTH ** -0.5, 1.0, ((1, 2),))
    group_gain = jnp.clip(1.0 + 0.18 * jax.random.normal(arg_keys[13], (CH,), jnp.float32), 0.099609375, 1.8984375).astype(jnp.bfloat16)
    head_proj = bell_draw(arg_keys[14], (HEADS * VDIM, D), (HEADS * VDIM // 16) ** -0.5, 0.75, ((0, 2), (1, 4)))
    channel_proj = bell_draw(arg_keys[15], (CH, D), CH ** -0.5, 0.1875, ((0, 2), (1, 4)))
    return {"tokens": tokens, "norm_gain": norm_gain, "query_down": query_down, "query_gain": query_gain, "latent_down": latent_down, "latent_gain": latent_gain, "rope_down": rope_down, "query_up": query_up, "key_up": key_up, "value_up": value_up, "glu_value": glu_value, "glu_gate": glu_gate, "conv_taps": conv_taps, "group_gain": group_gain, "head_proj": head_proj, "channel_proj": channel_proj}


norm_eps = 1e-06
rope_base = 10000.0

def rounded(values):
    return lax.optimization_barrier(values.astype(jnp.bfloat16))

def rms_scale(values, scale_gain):
    inv_rms = lax.rsqrt(lax.optimization_barrier(jnp.mean(values * values, axis=-1, keepdims=True)) + norm_eps)
    return values * inv_rms * scale_gain.astype(jnp.float32)

def angles_for(positions, rope_size):
    quarter = rope_size // 4
    inverse = rope_base ** (-jnp.arange(quarter, dtype=jnp.float32) / quarter)
    grid_row = (positions // GRID_W).astype(jnp.float32)
    grid_col = (positions % GRID_W).astype(jnp.float32)
    return jnp.concatenate([grid_row[:, None] * inverse, grid_col[:, None] * inverse], axis=-1)

def rotate(values, angles):
    half_size = values.shape[-1] // 2
    front_half = values[..., :half_size]
    back_half = values[..., half_size:]
    cosine = jnp.cos(angles)
    sine_part = jnp.sin(angles)
    return jnp.concatenate([front_half * cosine - back_half * sine_part, back_half * cosine + front_half * sine_part], axis=-1)

def reference(tokens, norm_gain, query_down, query_gain, latent_down, latent_gain, rope_down, query_up, key_up, value_up, glu_value, glu_gate, conv_taps, group_gain, head_proj, channel_proj):
    normed = rounded(rms_scale(tokens.astype(jnp.float32), norm_gain))
    positions = jnp.arange(LENGTH, dtype=jnp.int32)
    angles = angles_for(positions, ROPE)
    latent_query = rounded(rms_scale(jnp.dot(normed, query_down, preferred_element_type=jnp.float32), query_gain))
    query_all = jnp.dot(latent_query, query_up, preferred_element_type=jnp.float32).reshape(LENGTH, HEADS, NOPE + ROPE)
    query_plain = rounded(query_all[:, :, :NOPE])
    query_rope = rounded(rotate(query_all[:, :, NOPE:], angles[:, None, :]))
    absorbed = rounded(jnp.einsum('thd,rhd->htr', query_plain.astype(jnp.float32), key_up.astype(jnp.float32).reshape(KVR, HEADS, NOPE)))
    queries = jnp.concatenate([absorbed, jnp.transpose(query_rope, (1, 0, 2))], axis=-1).astype(jnp.float32)
    latent = rounded(rms_scale(jnp.dot(normed, latent_down, preferred_element_type=jnp.float32), latent_gain))
    rope_key = rounded(rotate(jnp.dot(normed, rope_down, preferred_element_type=jnp.float32), angles))
    keys = jnp.concatenate([latent, rope_key], axis=1).astype(jnp.float32)
    latent_wide = latent.astype(jnp.float32)
    score_scale = (NOPE + ROPE) ** (-0.5)
    block_count = LENGTH // TOK_DEV
    query_blocks = jnp.transpose(queries.reshape(HEADS, block_count, TOK_DEV, KVR + ROPE), (1, 0, 2, 3))

    def attend_block(query_block):
        scores = jnp.einsum('hqc,kc->hqk', query_block, keys) * score_scale
        row_max = lax.optimization_barrier(jnp.max(scores, axis=-1))
        weights = jnp.exp(scores - row_max[:, :, None])
        row_sum = lax.optimization_barrier(jnp.sum(weights, axis=-1))
        summed = jnp.einsum('hqk,kr->hqr', rounded(weights).astype(jnp.float32), latent_wide)
        return (rounded(summed / row_sum[:, :, None]), row_max + jnp.log(row_sum))
    attended, log_blocks = lax.map(attend_block, query_blocks)
    attended = jnp.transpose(attended, (1, 0, 2, 3)).reshape(HEADS, LENGTH, KVR)
    log_weight = jnp.transpose(log_blocks, (1, 0, 2)).reshape(HEADS, LENGTH)
    head_out = jnp.einsum('htr,rhv->thv', attended.astype(jnp.float32), value_up.astype(jnp.float32).reshape(KVR, HEADS, VDIM))
    head_out = rounded(head_out.reshape(LENGTH, HEADS * VDIM))
    value_in = jnp.dot(normed, glu_value, preferred_element_type=jnp.float32)
    gate_in = jnp.dot(normed, glu_gate, preferred_element_type=jnp.float32)
    gated_rows = rounded(value_in * jax.nn.sigmoid(gate_in))
    reach_rows = WIDTH // 2
    padded = jnp.pad(gated_rows.astype(jnp.float32), ((reach_rows, reach_rows), (0, 0)))
    filtered = padded[0:LENGTH] * conv_taps[0].astype(jnp.float32)
    for tap_index in range(1, WIDTH):
        filtered = filtered + padded[tap_index:tap_index + LENGTH] * conv_taps[tap_index].astype(jnp.float32)
    grouped = filtered.reshape(LENGTH, GROUPS, CH // GROUPS)
    centred = grouped - lax.optimization_barrier(jnp.mean(grouped, axis=-1, keepdims=True))
    spread = lax.optimization_barrier(jnp.mean(centred * centred, axis=-1, keepdims=True))
    normal_groups = (centred * lax.rsqrt(spread + norm_eps)).reshape(LENGTH, CH)
    conv_branch = rounded(jax.nn.silu(normal_groups * group_gain.astype(jnp.float32)))
    head_part = HEADS * VDIM // N_TP
    channel_part = CH // N_TP
    mixed_total = jnp.zeros((LENGTH, D), jnp.float32)
    for group_index in range(N_TP):
        head_lo = group_index * head_part
        chan_lo = group_index * channel_part
        partial_value = jnp.dot(head_out[:, head_lo:head_lo + head_part], head_proj[head_lo:head_lo + head_part], preferred_element_type=jnp.float32)
        partial_value = partial_value + jnp.dot(conv_branch[:, chan_lo:chan_lo + channel_part], channel_proj[chan_lo:chan_lo + channel_part], preferred_element_type=jnp.float32)
        mixed_total = mixed_total + rounded(partial_value).astype(jnp.float32)
    return (mixed_total.astype(jnp.bfloat16), log_weight)
```

```python
import functools

import jax
import jax.numpy as jnp
import numpy as np
from jax import lax
from jax.experimental import pallas as pl
from jax.experimental.pallas import tpu as pltpu
from jax.sharding import PartitionSpec as P

NOPE = 128
ROPE = 64
VDIM = 128
KVR = 256
CH = 1024
GROUPS = 8
GRID_W = 64


norm_eps = 1e-06
rope_base = 10000.0
far_below = -1e30


def padded_2(block, sides, width):
    for axis, dim in sides:
        count = lax.axis_size(axis)
        forward = [(i, i + 1) for i in range(count - 1)]
        backward = [(target, source) for source, target in forward]
        low = lax.ppermute(
            lax.slice_in_dim(block, block.shape[dim] - width, None, axis=dim), axis, forward
        )
        high = lax.ppermute(lax.slice_in_dim(block, 0, width, axis=dim), axis, backward)
        block = jnp.concatenate([low, block, high], axis=dim)
    return block


def rms_scale(values, scale_gain):
    inv_rms = lax.rsqrt(jnp.mean(values * values, axis=-1, keepdims=True) + norm_eps)
    return values * inv_rms * scale_gain.astype(jnp.float32)


def angles_for(positions, rope_size):
    quarter = rope_size // 4
    inverse = rope_base ** (-jnp.arange(quarter, dtype=jnp.float32) / quarter)
    grid_row = (positions // GRID_W).astype(jnp.float32)
    grid_col = (positions % GRID_W).astype(jnp.float32)
    return jnp.concatenate([grid_row[:, None] * inverse, grid_col[:, None] * inverse], axis=-1)


def rotate(values, angles):
    half_size = values.shape[-1] // 2
    front_half = values[..., :half_size]
    back_half = values[..., half_size:]
    cosine = jnp.cos(angles)
    sine_part = jnp.sin(angles)
    return jnp.concatenate(
        [front_half * cosine - back_half * sine_part, back_half * cosine + front_half * sine_part],
        axis=-1,
    )


def key_block(normed, latent_down, latent_gain, rope_down, positions):
    latent = jnp.dot(normed, latent_down, preferred_element_type=jnp.float32)
    latent = rms_scale(latent, latent_gain).astype(jnp.bfloat16)
    rope_key = jnp.dot(normed, rope_down, preferred_element_type=jnp.float32)
    rope_key = rotate(rope_key, angles_for(positions, rope_key.shape[-1])).astype(jnp.bfloat16)
    return jnp.concatenate([latent, rope_key], axis=1)


def per_device(
    tokens,
    norm_gain,
    query_down,
    query_gain,
    latent_down,
    latent_gain,
    rope_down,
    query_up,
    key_up,
    value_up,
    glu_value,
    glu_gate,
    conv_taps,
    group_gain,
    head_proj,
    channel_proj,
):
    tok_count = tokens.shape[0]
    reach_rows = conv_taps.shape[0] // 2
    head_count = key_up.shape[1] // NOPE
    normed = rms_scale(tokens.astype(jnp.float32), norm_gain).astype(jnp.bfloat16)
    offsets = lax.axis_index("sp") * tok_count + jnp.arange(tok_count, dtype=jnp.int32)
    query_latent = jnp.dot(
        normed,
        lax.all_gather(query_down, "sp", axis=0, tiled=True),
        preferred_element_type=jnp.float32,
    )
    value_in = jnp.dot(
        normed,
        lax.all_gather(glu_value, "sp", axis=0, tiled=True),
        preferred_element_type=jnp.float32,
    )
    gate_in = jnp.dot(
        normed,
        lax.all_gather(glu_gate, "sp", axis=0, tiled=True),
        preferred_element_type=jnp.float32,
    )
    latent_query = rms_scale(query_latent, query_gain).astype(jnp.bfloat16)
    query_all = jnp.dot(latent_query, query_up, preferred_element_type=jnp.float32).reshape(
        tok_count, head_count, NOPE + ROPE
    )
    query_plain = query_all[:, :, :NOPE].astype(jnp.bfloat16)
    query_rope = rotate(query_all[:, :, NOPE:], angles_for(offsets, ROPE)[:, None, :]).astype(
        jnp.bfloat16
    )
    absorbed = jnp.einsum(
        "thd,rhd->htr",
        query_plain,
        key_up.reshape(KVR, head_count, NOPE),
        preferred_element_type=jnp.float32,
    ).astype(jnp.bfloat16)
    queries = jnp.concatenate([absorbed, jnp.transpose(query_rope, (1, 0, 2))], axis=-1)
    score_scale = (NOPE + ROPE) ** (-0.5)
    half_rows = tok_count // lax.axis_size("tp")
    first_row = lax.axis_index("tp") * half_rows
    own_rows = lax.dynamic_slice_in_dim(normed, first_row, half_rows, 0)
    own_positions = lax.dynamic_slice_in_dim(offsets, first_row, half_rows, 0)
    own_keys = key_block(own_rows, latent_down, latent_gain, rope_down, own_positions)
    block_keys = lax.all_gather(own_keys, ("sp", "tp"), axis=0, tiled=True)
    row_max = jnp.full((head_count, tok_count), far_below, jnp.float32)
    scores = (
        jnp.einsum("hqc,kc->hqk", queries, block_keys, preferred_element_type=jnp.float32)
        * score_scale
    )
    new_max = jnp.maximum(row_max, jnp.max(scores, axis=2))
    weights = jnp.exp(scores - new_max[:, :, None])
    new_sum = jnp.sum(weights, axis=2)
    added = jnp.einsum(
        "hqk,kr->hqr",
        weights.astype(jnp.bfloat16),
        block_keys[:, :KVR],
        preferred_element_type=jnp.float32,
    )
    gated_rows = (value_in * jax.nn.sigmoid(gate_in)).astype(jnp.bfloat16)
    padded = padded_2(gated_rows, (("sp", 0),), reach_rows)
    filtered = padded[0:tok_count].astype(jnp.float32) * conv_taps[0].astype(jnp.float32)
    for tap_index in range(1, conv_taps.shape[0]):
        filtered = filtered + padded[tap_index : tap_index + tok_count].astype(
            jnp.float32
        ) * conv_taps[tap_index].astype(jnp.float32)
    grouped = filtered.reshape(tok_count, -1, CH // GROUPS)
    centred = grouped - jnp.mean(grouped, axis=-1, keepdims=True)
    spread = jnp.mean(centred * centred, axis=-1, keepdims=True)
    normal_groups = (centred * lax.rsqrt(spread + norm_eps)).reshape(tok_count, -1)
    conv_branch = jax.nn.silu(normal_groups * group_gain.astype(jnp.float32)).astype(jnp.bfloat16)
    attended = (added / new_sum[:, :, None]).astype(jnp.bfloat16)
    log_weight = new_max + jnp.log(new_sum)
    head_out = jnp.einsum(
        "htr,rhv->thv",
        attended,
        value_up.reshape(KVR, head_count, VDIM),
        preferred_element_type=jnp.float32,
    )
    head_out = head_out.reshape(tok_count, head_count * VDIM).astype(jnp.bfloat16)
    mixed_in = jnp.concatenate([head_out, conv_branch], axis=1)
    out_weight = jnp.concatenate([head_proj, channel_proj], axis=0)
    partial_terms = jnp.dot(
        mixed_in,
        lax.all_gather(out_weight, "sp", axis=1, tiled=True),
        preferred_element_type=jnp.float32,
    )
    mixed_out = lax.psum_scatter(
        partial_terms.astype(jnp.bfloat16), "tp", scatter_dimension=1, tiled=True
    )
    return (mixed_out, log_weight)


LANES = 128
MESH = pl.DeviceIdType.MESH
F32 = jnp.float32
BF16 = jnp.bfloat16
Z_IN, X_IN, Y_IN, DX_IN, DY_IN = range(5)
Z_LOW, Z_HIGH, Z_FWD, X_OUT, Y_OUT, DX_OUT, DY_OUT = range(7)


def rope_tables(length):
    quarter = ROPE // 4
    inverse = np.float32(rope_base) ** (-np.arange(quarter, dtype=np.float32) / np.float32(quarter))
    positions = np.arange(length)
    row = (positions // GRID_W).astype(np.float32)[:, None] * inverse
    col = (positions % GRID_W).astype(np.float32)[:, None] * inverse
    angles = np.concatenate([row, col], axis=1).astype(np.float32)
    cosine, sine = np.cos(angles), np.sin(angles)
    tables = np.zeros((3, length, LANES), np.float32)
    half = ROPE // 2
    tables[0, :, :half] = cosine
    tables[0, :, half:ROPE] = cosine
    tables[1, :, :half] = -sine
    tables[2, :, half:ROPE] = sine
    return tables


def dot(a, b):
    return jnp.dot(a, b, preferred_element_type=F32)


def dot_nt(a, b):
    return lax.dot_general(a, b, (((1,), (1,)), ((), ())), preferred_element_type=F32)


def fused_kernel(
    n_sp,
    tokens, norm_gain, query_down, query_gain, latent_down, latent_gain, rope_down, query_up,
    key_up, value_up, glu_value, glu_gate, conv_taps, group_gain, head_proj, channel_proj, tables,
    out, log_out,
    w_q, w_g, w_o, tok_v, lat_v, rope_v, qup_v, kup_v, vup_v, tab_v,
    normed, keys, key_tmp, q_acc, q_lat, q_scr, g_acc, mixed, gated, low_rows, high_rows, padded,
    parts, peer_parts,
    load_sem, recv_sem, send_sem, key_recv, key_send, pair_recv, pair_send, halo_recv, halo_send,
):
    z = lax.axis_index("sp")
    c = lax.axis_index("fs")
    t = lax.axis_index("tp")
    peer = 1 - t
    c_x = c + 1 - 2 * (c % 2)
    c_y = (c + 2) % 4
    c_d = 3 - c
    rows = tokens.shape[0]
    depth = query_down.shape[0]
    q_cols = w_q.shape[2]
    chans = glu_value.shape[1]
    heads = key_up.shape[1] // NOPE
    head_rows = head_proj.shape[0]
    out_rows = w_o.shape[1]

    loads = {}

    def load(name, src, dst):
        copy = pltpu.make_async_copy(src, dst, load_sem.at[len(loads)])
        copy.start()
        loads[name] = copy

    load("wq", query_down.at[:, pl.ds(pl.multiple_of(t * q_cols, LANES), q_cols)], w_q.at[z])
    load("gv", glu_value, w_g.at[z, :, pl.ds(0, chans)])
    load("gg", glu_gate, w_g.at[z, :, pl.ds(chans, chans)])
    load("tok", tokens, tok_v)
    load("lat", latent_down, lat_v)
    load("rope", rope_down, rope_v)
    load("tab", tables.at[:, pl.ds(pl.multiple_of(z * rows, LANES), rows), :], tab_v)
    load("hp", head_proj, w_o.at[z, pl.ds(0, head_rows), :])
    load("cp", channel_proj, w_o.at[z, pl.ds(head_rows, out_rows - head_rows), :])
    load("qup", query_up, qup_v)
    load("kup", key_up, kup_v)
    load("vup", value_up, vup_v)

    barrier = pltpu.get_barrier_semaphore()
    partners = [{"sp": (z + d) % n_sp} for d in range(1, n_sp)]
    partners += [{"fs": c_x}, {"fs": c_y}, {"tp": peer}]
    for partner in partners:
        pl.semaphore_signal(barrier, inc=1, device_id=partner, device_id_type=MESH)
    pl.semaphore_wait(barrier, len(partners))

    direct_rows = (out_rows // 4) // 64 * 64
    units = [
        (w_q, 0, depth, True),
        (w_g, 0, depth, True),
        (w_o, 0, out_rows - direct_rows, True),
        (w_o, out_rows - direct_rows, direct_rows, False),
    ]
    Q, G, O, D = range(4)

    def block(u, shard, quarter, half=None):
        buf, first, count, shared = units[u]
        if not shared:
            return buf.at[shard, pl.ds(first, count), :]
        size = count // 4
        start = first + quarter * size
        if half is not None:
            size = size // 2
            start = start + half * size
        return buf.at[shard, pl.ds(pl.multiple_of(start, 16), size), :]

    def remote(u, shard, ref, out_kind, in_kind, device):
        return pltpu.make_async_remote_copy(
            src_ref=ref, dst_ref=ref,
            send_sem=send_sem.at[u, shard, out_kind], recv_sem=recv_sem.at[u, shard, in_kind],
            device_id=device, device_id_type=MESH,
        )

    def own_copy(u, low):
        return remote(
            u, z, block(u, z, c), Z_LOW if low else Z_HIGH, Z_IN, {"sp": z - 1 if low else z + 1}
        )

    def send_own(u):
        @pl.when(z > 0)
        def _():
            own_copy(u, True).start()

        @pl.when(z < n_sp - 1)
        def _():
            own_copy(u, False).start()

    nearest = jnp.minimum(z, n_sp - 1 - z)
    arrivals = []
    for k in range(n_sp - 1):
        both = k < 2 * nearest
        distance = jnp.where(both, k // 2 + 1, k - nearest + 1)
        from_low = jnp.where(both, 1 - k % 2, (2 * z > n_sp - 1).astype(jnp.int32))
        shard = z - distance * (2 * from_low - 1)
        arrivals.append((shard, z + 2 * from_low - 1))

    def forward_copy(u, k):
        shard, target = arrivals[k]
        return remote(u, shard, block(u, shard, c), Z_FWD, Z_IN, {"sp": target})

    def when_forward(k, action):
        target = arrivals[k][1]

        @pl.when((target >= 0) & (target < n_sp))
        def _():
            action()

    def side_copies(u, k):
        shard, _ = arrivals[k]
        mine = block(u, shard, c)
        return (
            remote(u, shard, mine, X_OUT, X_IN, {"fs": c_x}),
            remote(u, shard, mine, Y_OUT, Y_IN, {"fs": c_y}),
        )

    def corner_copies(u, k):
        shard, _ = arrivals[k]
        return (
            remote(u, shard, block(u, shard, c_x, 0), DY_OUT, DY_IN, {"fs": c_y}),
            remote(u, shard, block(u, shard, c_y, 1), DX_OUT, DX_IN, {"fs": c_x}),
        )

    def wait_in(u, k, kind, quarter, half=None):
        shard, _ = arrivals[k]
        remote(u, shard, block(u, shard, quarter, half), Z_FWD, kind, {"fs": c_x}).wait_recv()

    def step_a(u, k):
        wait_in(u, k, Z_IN, c)
        when_forward(k, lambda: forward_copy(u, k).start())
        if units[u][3]:
            for copy in side_copies(u, k):
                copy.start()

    def step_b(u, k):
        to_y, to_x = corner_copies(u, k)
        wait_in(u, k, X_IN, c_x)
        to_y.start()
        wait_in(u, k, Y_IN, c_y)
        to_x.start()

    def step_c(u, k):
        wait_in(u, k, DY_IN, c_d, 0)
        wait_in(u, k, DX_IN, c_d, 1)

    loads["wq"].wait()
    send_own(Q)
    loads["gv"].wait()
    loads["gg"].wait()
    send_own(G)

    loads["tok"].wait()
    values = tok_v[...].astype(F32)
    normed[...] = rms_scale(values, norm_gain[...]).astype(BF16)

    def rotate_lanes(v):
        half = ROPE // 2
        return (
            v * tab_v[0] + pltpu.roll(v, LANES - half, 1) * tab_v[1] + pltpu.roll(v, half, 1) * tab_v[2]
        )

    loads["lat"].wait()
    latent = rms_scale(dot(normed[...], lat_v[...]), latent_gain[...])
    keys[z, :, 0:KVR] = latent.astype(BF16)
    loads["rope"].wait()
    loads["tab"].wait()
    key_tmp[...] = jnp.zeros_like(key_tmp)
    key_tmp[:, 0:ROPE] = dot(normed[...], rope_v[...])
    keys[z, :, KVR : KVR + LANES] = rotate_lanes(key_tmp[...]).astype(BF16)

    def key_copy(d):
        return pltpu.make_async_remote_copy(
            src_ref=keys.at[z], dst_ref=keys.at[z],
            send_sem=key_send.at[d], recv_sem=key_recv.at[d],
            device_id={"sp": (z + d) % n_sp}, device_id_type=MESH,
        )

    def key_arrival(d):
        source = (z + n_sp - d) % n_sp
        return pltpu.make_async_remote_copy(
            src_ref=keys.at[source], dst_ref=keys.at[source],
            send_sem=key_send.at[d], recv_sem=key_recv.at[d],
            device_id={"sp": source}, device_id_type=MESH,
        )

    for d in range(1, n_sp):
        key_copy(d).start()

    def add_shard(acc, weights, shard, first=False):
        columns = pl.ds(pl.multiple_of(shard * depth, LANES), depth)
        term = dot(normed[:, columns], weights[shard])
        acc[...] = term if first else acc[...] + term

    add_shard(q_acc, w_q, z, True)
    add_shard(g_acc, w_g, z, True)

    last = n_sp - 2
    loads["hp"].wait()
    loads["cp"].wait()
    for k in range(last + 1):
        step_a(Q, k)
        if k:
            step_b(Q, k - 1)
        if k > 1:
            step_c(Q, k - 2)
            add_shard(q_acc, w_q, arrivals[k - 2][0])
    send_own(O)
    step_b(Q, last)
    step_a(G, 0)
    for k in range(max(last - 1, 0), last + 1):
        step_c(Q, k)
        add_shard(q_acc, w_q, arrivals[k][0])

    q_lat[t] = q_acc[...]
    q_copy = pltpu.make_async_remote_copy(
        src_ref=q_lat.at[t], dst_ref=q_lat.at[t], send_sem=pair_send.at[0], recv_sem=pair_recv.at[0],
        device_id={"tp": peer}, device_id_type=MESH,
    )
    q_copy.start()
    loads["qup"].wait()
    loads["kup"].wait()
    loads["vup"].wait()
    pltpu.make_async_remote_copy(
        src_ref=q_lat.at[peer], dst_ref=q_lat.at[peer], send_sem=pair_send.at[0],
        recv_sem=pair_recv.at[0], device_id={"tp": peer}, device_id_type=MESH,
    ).wait_recv()
    whole_q = jnp.concatenate([q_lat[0], q_lat[1]], axis=1)
    latent_query = rms_scale(whole_q, query_gain[...]).astype(BF16)
    q_scr[...] = dot(latent_query, qup_v[...])
    for d in range(1, n_sp):
        key_arrival(d).wait_recv()

    def attend(h, shifted):
        start = h * (NOPE + ROPE)
        source = q_scr[...]
        if start % LANES:
            source, start = shifted, start - ROPE
        plain = source[:, start : start + NOPE].astype(BF16)
        rope_part = rotate_lanes(source[:, start + NOPE : start + NOPE + LANES]).astype(BF16)
        absorbed = dot_nt(plain, kup_v[:, h * NOPE : (h + 1) * NOPE]).astype(BF16)
        query = jnp.concatenate([absorbed, rope_part], axis=1)
        all_keys = keys[...].reshape(n_sp * rows, KVR + LANES)
        scores = dot_nt(query, all_keys) * (NOPE + ROPE) ** (-0.5)
        row_max = jnp.max(scores, axis=1, keepdims=True)
        weights = jnp.exp(scores - row_max)
        total = jnp.sum(weights, axis=1, keepdims=True)
        added = dot(weights.astype(BF16), all_keys[:, 0:KVR])
        attended = (added / total).astype(BF16)
        head_out = dot(attended, vup_v[:, h * VDIM : (h + 1) * VDIM])
        mixed[:, h * VDIM : (h + 1) * VDIM] = head_out.astype(BF16)
        return row_max + jnp.log(total)

    whole = q_scr[...]
    shifted = pltpu.roll(whole, whole.shape[1] - ROPE, 1)
    lane = lax.broadcasted_iota(jnp.int32, (rows, LANES), 1)
    logs = jnp.zeros((rows, LANES), F32)
    relays = [lambda: step_a(G, 1), lambda: step_b(G, 0), lambda: step_a(G, 2), lambda: None]
    if n_sp == 2:
        relays = [lambda: step_b(G, 0)]
    for h in range(heads):
        logs = jnp.where(lane == h, attend(h, shifted), logs)
        if h < len(relays):
            relays[h]()
    for h in range(heads, len(relays)):
        relays[h]()
    log_out[...] = jnp.transpose(logs)[0:heads, :]

    send_own(D)
    if n_sp > 2:
        step_b(G, 1)
        step_c(G, 0)
        add_shard(g_acc, w_g, arrivals[0][0])
        step_a(O, 0)
        step_b(G, 2)
        step_c(G, 1)
        add_shard(g_acc, w_g, arrivals[1][0])
        step_a(O, 1)
        step_c(G, 2)
        add_shard(g_acc, w_g, arrivals[2][0])
    else:
        step_a(O, 0)
        step_c(G, 0)
        add_shard(g_acc, w_g, arrivals[0][0])

    halo = low_rows.shape[0]
    reach = conv_taps.shape[0] // 2
    gated[...] = (g_acc[:, 0:chans] * jax.nn.sigmoid(g_acc[:, chans : 2 * chans])).astype(BF16)
    up_copy = pltpu.make_async_remote_copy(
        src_ref=gated.at[pl.ds(rows - halo, halo), :], dst_ref=low_rows,
        send_sem=halo_send.at[0], recv_sem=halo_recv.at[0],
        device_id={"sp": z + 1}, device_id_type=MESH,
    )
    down_copy = pltpu.make_async_remote_copy(
        src_ref=gated.at[pl.ds(0, halo), :], dst_ref=high_rows,
        send_sem=halo_send.at[1], recv_sem=halo_recv.at[1],
        device_id={"sp": z - 1}, device_id_type=MESH,
    )

    @pl.when(z < n_sp - 1)
    def _():
        up_copy.start()

    @pl.when(z > 0)
    def _():
        down_copy.start()

    padded[halo : halo + rows, :] = gated[...].astype(F32)
    step_b(O, 0)
    if n_sp > 2:
        step_a(O, 2)

    @pl.when(z > 0)
    def _():
        up_copy.wait_recv()
        padded[0:halo, :] = low_rows[...].astype(F32)

    @pl.when(z == 0)
    def _():
        padded[0:halo, :] = jnp.zeros((halo, chans), F32)

    @pl.when(z < n_sp - 1)
    def _():
        down_copy.wait_recv()
        padded[halo + rows : 2 * halo + rows, :] = high_rows[...].astype(F32)

    @pl.when(z == n_sp - 1)
    def _():
        padded[halo + rows : 2 * halo + rows, :] = jnp.zeros((halo, chans), F32)

    group = CH // GROUPS
    for g in range(chans // group):
        lanes = slice(g * group, (g + 1) * group)
        taps = conv_taps[:, lanes].astype(F32)
        filtered = jnp.zeros((rows, group), F32)
        for j in range(conv_taps.shape[0]):
            first = halo - reach + j
            filtered = filtered + padded[first : first + rows, lanes] * taps[j : j + 1, :]
        centred = filtered - jnp.mean(filtered, axis=1, keepdims=True)
        spread = jnp.mean(centred * centred, axis=1, keepdims=True)
        branch = centred * lax.rsqrt(spread + norm_eps) * group_gain[:, lanes].astype(F32)
        branch = branch * jax.nn.sigmoid(branch)
        mixed[:, heads * VDIM + g * group : heads * VDIM + (g + 1) * group] = branch.astype(BF16)
        if g == 0 and n_sp > 2:
            step_b(O, 1)
        if g == 2:
            step_c(O, 0)
            step_a(D, 0)

    def add_part(shard):
        parts[shard] = dot(mixed[...], w_o[shard]).astype(BF16)

    add_part(z)
    if n_sp > 2:
        step_a(D, 1)
        add_part(arrivals[0][0])
        step_b(O, 2)
        step_c(O, 1)
        step_a(D, 2)
        add_part(arrivals[1][0])
        step_c(O, 2)
        add_part(arrivals[2][0])
    else:
        add_part(arrivals[0][0])

    half_sp = n_sp // 2
    p_copy = pltpu.make_async_remote_copy(
        src_ref=parts.at[pl.ds(peer * half_sp, half_sp)], dst_ref=peer_parts,
        send_sem=pair_send.at[1], recv_sem=pair_recv.at[1],
        device_id={"tp": peer}, device_id_type=MESH,
    )
    p_copy.start()

    for u in range(len(units)):
        @pl.when(z > 0)
        def _():
            own_copy(u, True).wait_send()

        @pl.when(z < n_sp - 1)
        def _():
            own_copy(u, False).wait_send()

        for k in range(n_sp - 1):
            when_forward(k, lambda: forward_copy(u, k).wait_send())
            if units[u][3]:
                for copy in side_copies(u, k) + corner_copies(u, k):
                    copy.wait_send()
    for d in range(1, n_sp):
        key_copy(d).wait_send()
    q_copy.wait_send()

    @pl.when(z < n_sp - 1)
    def _():
        up_copy.wait_send()

    @pl.when(z > 0)
    def _():
        down_copy.wait_send()

    p_copy.wait()
    width = parts.shape[2]
    for i in range(half_sp):
        total = parts[t * half_sp + i].astype(F32) + peer_parts[i].astype(F32)
        out[:, i * width : (i + 1) * width] = total.astype(BF16)


def fused_device(n_sp, *args):
    (tokens, norm_gain, query_down, query_gain, latent_down, latent_gain, rope_down, query_up,
     key_up, value_up, glu_value, glu_gate, conv_taps, group_gain, head_proj, channel_proj) = args
    rows, width = tokens.shape
    depth, q_rank = query_down.shape
    chans = glu_value.shape[1]
    heads = key_up.shape[1] // NOPE
    out_rows = head_proj.shape[0] + channel_proj.shape[0]
    cols = head_proj.shape[1]
    halo = (conv_taps.shape[0] // 2 + 15) // 16 * 16
    tables = jnp.asarray(rope_tables(n_sp * rows))
    vmem = pl.BlockSpec(memory_space=pltpu.VMEM)
    hbm = pl.BlockSpec(memory_space=pl.ANY)
    as_row = lambda v: v.reshape(1, -1)
    operands = [
        (tokens, hbm), (as_row(norm_gain), vmem), (query_down, hbm), (as_row(query_gain), vmem),
        (latent_down, hbm), (as_row(latent_gain), vmem), (rope_down, hbm), (query_up, hbm),
        (key_up, hbm), (value_up, hbm), (glu_value, hbm), (glu_gate, hbm), (conv_taps, vmem),
        (as_row(group_gain), vmem), (head_proj, hbm), (channel_proj, hbm), (tables, hbm),
    ]
    like = lambda a: pltpu.VMEM(a.shape, a.dtype)
    dma = pltpu.SemaphoreType.DMA
    scratch = [
        pltpu.VMEM((n_sp, depth, q_rank // 2), BF16),
        pltpu.VMEM((n_sp, depth, 2 * chans), BF16),
        pltpu.VMEM((n_sp, out_rows, cols), BF16),
        like(tokens), like(latent_down), like(rope_down), like(query_up), like(key_up), like(value_up),
        pltpu.VMEM((3, rows, LANES), F32),
        pltpu.VMEM((rows, width), BF16),
        pltpu.VMEM((n_sp, rows, KVR + LANES), BF16),
        pltpu.VMEM((rows, LANES), F32),
        pltpu.VMEM((rows, q_rank // 2), F32),
        pltpu.VMEM((2, rows, q_rank // 2), F32),
        pltpu.VMEM((rows, query_up.shape[1]), F32),
        pltpu.VMEM((rows, 2 * chans), F32),
        pltpu.VMEM((rows, out_rows), BF16),
        pltpu.VMEM((rows, chans), BF16),
        pltpu.VMEM((halo, chans), BF16),
        pltpu.VMEM((halo, chans), BF16),
        pltpu.VMEM((rows + 2 * halo, chans), F32),
        pltpu.VMEM((n_sp, rows, cols), BF16),
        pltpu.VMEM((n_sp // 2, rows, cols), BF16),
        dma((12,)), dma((4, n_sp, 5)), dma((4, n_sp, 7)), dma((n_sp,)), dma((n_sp,)),
        dma((2,)), dma((2,)), dma((2,)), dma((2,)),
    ]
    return pl.pallas_call(
        functools.partial(fused_kernel, n_sp),
        out_shape=(
            jax.ShapeDtypeStruct((rows, n_sp * cols // 2), BF16),
            jax.ShapeDtypeStruct((heads, rows), F32),
        ),
        in_specs=[spec for _, spec in operands],
        out_specs=(vmem, vmem),
        scratch_shapes=scratch,
        compiler_params=pltpu.CompilerParams(
            collective_id=0, has_side_effects=True, vmem_limit_bytes=48 * 1024 * 1024
        ),
        name="fused_layer",
    )(*[value for value, _ in operands])


def solution(mesh):
    in_specs = (
        P(("fs", "sp"), None),
        P(),
        P("sp", None),
        P(),
        P(),
        P(),
        P(),
        P(None, "tp"),
        P(None, "tp"),
        P(None, "tp"),
        P("sp", "tp"),
        P("sp", "tp"),
        P(None, "tp"),
        P("tp"),
        P("tp", "sp"),
        P("tp", "sp"),
    )
    out_specs = (P(("fs", "sp"), "tp"), P("tp", ("fs", "sp")))
    body = per_device
    if mesh.shape["fs"] == 4 and mesh.shape["tp"] == 2 and mesh.shape["sp"] in (2, 4):
        body = functools.partial(fused_device, mesh.shape["sp"])
    return jax.shard_map(
        body, mesh=mesh, in_specs=in_specs, out_specs=out_specs, check_vma=False
    )
```

```python
import functools

import jax
import jax.numpy as jnp
import numpy as np
from jax import lax
from jax.experimental import pallas as pl
from jax.experimental.pallas import tpu as pltpu
from jax.sharding import PartitionSpec as P

NOPE = 128
ROPE = 64
VDIM = 128
KVR = 256
CH = 1024
GROUPS = 8
GRID_W = 64


norm_eps = 1e-06
rope_base = 10000.0
far_below = -1e30


def padded_2(block, sides, width):
    for axis, dim in sides:
        count = lax.axis_size(axis)
        forward = [(i, i + 1) for i in range(count - 1)]
        backward = [(target, source) for source, target in forward]
        low = lax.ppermute(
            lax.slice_in_dim(block, block.shape[dim] - width, None, axis=dim), axis, forward
        )
        high = lax.ppermute(lax.slice_in_dim(block, 0, width, axis=dim), axis, backward)
        block = jnp.concatenate([low, block, high], axis=dim)
    return block


def rms_scale(values, scale_gain):
    inv_rms = lax.rsqrt(jnp.mean(values * values, axis=-1, keepdims=True) + norm_eps)
    return values * inv_rms * scale_gain.astype(jnp.float32)


def angles_for(positions, rope_size):
    quarter = rope_size // 4
    inverse = rope_base ** (-jnp.arange(quarter, dtype=jnp.float32) / quarter)
    grid_row = (positions // GRID_W).astype(jnp.float32)
    grid_col = (positions % GRID_W).astype(jnp.float32)
    return jnp.concatenate([grid_row[:, None] * inverse, grid_col[:, None] * inverse], axis=-1)


def rotate(values, angles):
    half_size = values.shape[-1] // 2
    front_half = values[..., :half_size]
    back_half = values[..., half_size:]
    cosine = jnp.cos(angles)
    sine_part = jnp.sin(angles)
    return jnp.concatenate(
        [front_half * cosine - back_half * sine_part, back_half * cosine + front_half * sine_part],
        axis=-1,
    )


def key_block(normed, latent_down, latent_gain, rope_down, positions):
    latent = jnp.dot(normed, latent_down, preferred_element_type=jnp.float32)
    latent = rms_scale(latent, latent_gain).astype(jnp.bfloat16)
    rope_key = jnp.dot(normed, rope_down, preferred_element_type=jnp.float32)
    rope_key = rotate(rope_key, angles_for(positions, rope_key.shape[-1])).astype(jnp.bfloat16)
    return jnp.concatenate([latent, rope_key], axis=1)


def per_device(
    tokens,
    norm_gain,
    query_down,
    query_gain,
    latent_down,
    latent_gain,
    rope_down,
    query_up,
    key_up,
    value_up,
    glu_value,
    glu_gate,
    conv_taps,
    group_gain,
    head_proj,
    channel_proj,
):
    tok_count = tokens.shape[0]
    reach_rows = conv_taps.shape[0] // 2
    head_count = key_up.shape[1] // NOPE
    normed = rms_scale(tokens.astype(jnp.float32), norm_gain).astype(jnp.bfloat16)
    offsets = lax.axis_index("sp") * tok_count + jnp.arange(tok_count, dtype=jnp.int32)
    query_latent = jnp.dot(
        normed,
        lax.all_gather(query_down, "sp", axis=0, tiled=True),
        preferred_element_type=jnp.float32,
    )
    value_in = jnp.dot(
        normed,
        lax.all_gather(glu_value, "sp", axis=0, tiled=True),
        preferred_element_type=jnp.float32,
    )
    gate_in = jnp.dot(
        normed,
        lax.all_gather(glu_gate, "sp", axis=0, tiled=True),
        preferred_element_type=jnp.float32,
    )
    latent_query = rms_scale(query_latent, query_gain).astype(jnp.bfloat16)
    query_all = jnp.dot(latent_query, query_up, preferred_element_type=jnp.float32).reshape(
        tok_count, head_count, NOPE + ROPE
    )
    query_plain = query_all[:, :, :NOPE].astype(jnp.bfloat16)
    query_rope = rotate(query_all[:, :, NOPE:], angles_for(offsets, ROPE)[:, None, :]).astype(
        jnp.bfloat16
    )
    absorbed = jnp.einsum(
        "thd,rhd->htr",
        query_plain,
        key_up.reshape(KVR, head_count, NOPE),
        preferred_element_type=jnp.float32,
    ).astype(jnp.bfloat16)
    queries = jnp.concatenate([absorbed, jnp.transpose(query_rope, (1, 0, 2))], axis=-1)
    score_scale = (NOPE + ROPE) ** (-0.5)
    half_rows = tok_count // lax.axis_size("tp")
    first_row = lax.axis_index("tp") * half_rows
    own_rows = lax.dynamic_slice_in_dim(normed, first_row, half_rows, 0)
    own_positions = lax.dynamic_slice_in_dim(offsets, first_row, half_rows, 0)
    own_keys = key_block(own_rows, latent_down, latent_gain, rope_down, own_positions)
    block_keys = lax.all_gather(own_keys, ("sp", "tp"), axis=0, tiled=True)
    row_max = jnp.full((head_count, tok_count), far_below, jnp.float32)
    scores = (
        jnp.einsum("hqc,kc->hqk", queries, block_keys, preferred_element_type=jnp.float32)
        * score_scale
    )
    new_max = jnp.maximum(row_max, jnp.max(scores, axis=2))
    weights = jnp.exp(scores - new_max[:, :, None])
    new_sum = jnp.sum(weights, axis=2)
    added = jnp.einsum(
        "hqk,kr->hqr",
        weights.astype(jnp.bfloat16),
        block_keys[:, :KVR],
        preferred_element_type=jnp.float32,
    )
    gated_rows = (value_in * jax.nn.sigmoid(gate_in)).astype(jnp.bfloat16)
    padded = padded_2(gated_rows, (("sp", 0),), reach_rows)
    filtered = padded[0:tok_count].astype(jnp.float32) * conv_taps[0].astype(jnp.float32)
    for tap_index in range(1, conv_taps.shape[0]):
        filtered = filtered + padded[tap_index : tap_index + tok_count].astype(
            jnp.float32
        ) * conv_taps[tap_index].astype(jnp.float32)
    grouped = filtered.reshape(tok_count, -1, CH // GROUPS)
    centred = grouped - jnp.mean(grouped, axis=-1, keepdims=True)
    spread = jnp.mean(centred * centred, axis=-1, keepdims=True)
    normal_groups = (centred * lax.rsqrt(spread + norm_eps)).reshape(tok_count, -1)
    conv_branch = jax.nn.silu(normal_groups * group_gain.astype(jnp.float32)).astype(jnp.bfloat16)
    attended = (added / new_sum[:, :, None]).astype(jnp.bfloat16)
    log_weight = new_max + jnp.log(new_sum)
    head_out = jnp.einsum(
        "htr,rhv->thv",
        attended,
        value_up.reshape(KVR, head_count, VDIM),
        preferred_element_type=jnp.float32,
    )
    head_out = head_out.reshape(tok_count, head_count * VDIM).astype(jnp.bfloat16)
    mixed_in = jnp.concatenate([head_out, conv_branch], axis=1)
    out_weight = jnp.concatenate([head_proj, channel_proj], axis=0)
    partial_terms = jnp.dot(
        mixed_in,
        lax.all_gather(out_weight, "sp", axis=1, tiled=True),
        preferred_element_type=jnp.float32,
    )
    mixed_out = lax.psum_scatter(
        partial_terms.astype(jnp.bfloat16), "tp", scatter_dimension=1, tiled=True
    )
    return (mixed_out, log_weight)


LANES = 128
MESH = pl.DeviceIdType.MESH
F32 = jnp.float32
BF16 = jnp.bfloat16
Z_IN, X_IN, Y_IN, DX_IN, DY_IN = range(5)
Z_LOW, Z_HIGH, Z_FWD, X_OUT, Y_OUT, DX_OUT, DY_OUT = range(7)


def rope_tables(length):
    quarter = ROPE // 4
    inverse = np.float32(rope_base) ** (-np.arange(quarter, dtype=np.float32) / np.float32(quarter))
    positions = np.arange(length)
    row = (positions // GRID_W).astype(np.float32)[:, None] * inverse
    col = (positions % GRID_W).astype(np.float32)[:, None] * inverse
    angles = np.concatenate([row, col], axis=1).astype(np.float32)
    cosine, sine = np.cos(angles), np.sin(angles)
    tables = np.zeros((3, length, LANES), np.float32)
    half = ROPE // 2
    tables[0, :, :half] = cosine
    tables[0, :, half:ROPE] = cosine
    tables[1, :, :half] = -sine
    tables[2, :, half:ROPE] = sine
    return tables


def dot(a, b):
    return jnp.dot(a, b, preferred_element_type=F32)


def row_of(ref):
    return ref[...].reshape(1, -1)


def dot_nt(a, b):
    return lax.dot_general(a, b, (((1,), (1,)), ((), ())), preferred_element_type=F32)


def fused_kernel(
    n_sp,
    tokens, norm_gain, query_down, query_gain, latent_down, latent_gain, rope_down, query_up,
    key_up, value_up, glu_value, glu_gate, conv_taps, group_gain, head_proj, channel_proj, tables,
    out, log_out,
    w_q, w_v, w_t, w_o, tok_v, lat_v, rope_v, qup_v, kup_v, vup_v, tab_v,
    normed, keys, key_tmp, q_acc, q_lat, q_scr, v_acc, t_acc, mixed, gated, low_rows, high_rows, padded,
    parts, peer_parts,
    load_sem, recv_sem, send_sem, key_recv, key_send, key_pair_recv, key_pair_send, pair_recv, pair_send, halo_recv, halo_send,
):
    z = lax.axis_index("sp")
    c = lax.axis_index("fs")
    t = lax.axis_index("tp")
    peer = 1 - t
    c_x = c + 1 - 2 * (c % 2)
    c_y = (c + 2) % 4
    c_d = 3 - c
    rows = tokens.shape[0]
    depth = query_down.shape[0]
    q_cols = w_q.shape[2]
    chans = glu_value.shape[1]
    heads = key_up.shape[1] // NOPE
    head_rows = head_proj.shape[0]
    out_rows = w_o.shape[1]

    loads = {}

    def load(name, src, dst):
        copy = pltpu.make_async_copy(src, dst, load_sem.at[len(loads)])
        copy.start()
        loads[name] = copy

    load("wq", query_down.at[:, pl.ds(pl.multiple_of(t * q_cols, LANES), q_cols)], w_q.at[z])
    load("gv", glu_value, w_v.at[z])
    load("gg", glu_gate, w_t.at[z])
    load("tok", tokens, tok_v)
    load("lat", latent_down, lat_v)
    load("rope", rope_down, rope_v)
    load("tab", tables.at[:, pl.ds(pl.multiple_of(z * rows, LANES), rows), :], tab_v)
    load("hp", head_proj, w_o.at[z, pl.ds(0, head_rows), :])
    load("cp", channel_proj, w_o.at[z, pl.ds(head_rows, out_rows - head_rows), :])
    load("qup", query_up, qup_v)
    load("kup", key_up, kup_v)
    load("vup", value_up, vup_v)

    barrier = pltpu.get_barrier_semaphore()
    sides = [{"fs": c_x}, {"fs": c_y}, {"tp": peer}]
    for partner in sides:
        pl.semaphore_signal(barrier, inc=1, device_id=partner, device_id_type=MESH)

    @pl.when(z > 0)
    def _():
        pl.semaphore_signal(barrier, inc=1, device_id={"sp": z - 1}, device_id_type=MESH)

    @pl.when(z < n_sp - 1)
    def _():
        pl.semaphore_signal(barrier, inc=1, device_id={"sp": z + 1}, device_id_type=MESH)

    ends = (z == 0).astype(jnp.int32) + (z == n_sp - 1).astype(jnp.int32)
    pl.semaphore_wait(barrier, len(sides) + 2 - ends)

    direct_rows = (out_rows // 4) // 64 * 64
    units = [
        (w_q, 0, depth, True),
        (w_v, 0, depth, True),
        (w_t, 0, depth, True),
        (w_o, 0, head_rows, True),
        (w_o, head_rows, out_rows - head_rows - direct_rows, True),
        (w_o, out_rows - direct_rows, direct_rows, False),
    ]
    Q, V, T, H, P, D = range(6)

    def block(u, shard, quarter, half=None):
        buf, first, count, shared = units[u]
        if not shared:
            return buf.at[shard, pl.ds(first, count), :]
        size = count // 4
        start = first + quarter * size
        if half is not None:
            size = size // 2
            start = start + half * size
        return buf.at[shard, pl.ds(pl.multiple_of(start, 16), size), :]

    def remote(u, shard, ref, out_kind, in_kind, device):
        return pltpu.make_async_remote_copy(
            src_ref=ref, dst_ref=ref,
            send_sem=send_sem.at[u, shard, out_kind], recv_sem=recv_sem.at[u, shard, in_kind],
            device_id=device, device_id_type=MESH,
        )

    def own_copy(u, low):
        return remote(
            u, z, block(u, z, c), Z_LOW if low else Z_HIGH, Z_IN, {"sp": z - 1 if low else z + 1}
        )

    def send_own(u):
        @pl.when(z > 0)
        def _():
            own_copy(u, True).start()

        @pl.when(z < n_sp - 1)
        def _():
            own_copy(u, False).start()

    nearest = jnp.minimum(z, n_sp - 1 - z)
    arrivals = []
    for k in range(n_sp - 1):
        both = k < 2 * nearest
        distance = jnp.where(both, k // 2 + 1, k - nearest + 1)
        from_low = jnp.where(both, 1 - k % 2, (2 * z > n_sp - 1).astype(jnp.int32))
        shard = z - distance * (2 * from_low - 1)
        arrivals.append((shard, z + 2 * from_low - 1))

    def forward_copy(u, k):
        shard, target = arrivals[k]
        return remote(u, shard, block(u, shard, c), Z_FWD, Z_IN, {"sp": target})

    def when_forward(k, action):
        target = arrivals[k][1]

        @pl.when((target >= 0) & (target < n_sp))
        def _():
            action()

    def side_copies(u, k):
        shard, _ = arrivals[k]
        mine = block(u, shard, c)
        return (
            remote(u, shard, mine, X_OUT, X_IN, {"fs": c_x}),
            remote(u, shard, mine, Y_OUT, Y_IN, {"fs": c_y}),
        )

    def corner_copies(u, k):
        shard, _ = arrivals[k]
        return (
            remote(u, shard, block(u, shard, c_x, 0), DY_OUT, DY_IN, {"fs": c_y}),
            remote(u, shard, block(u, shard, c_y, 1), DX_OUT, DX_IN, {"fs": c_x}),
        )

    def wait_in(u, k, kind, quarter, half=None):
        shard, _ = arrivals[k]
        remote(u, shard, block(u, shard, quarter, half), Z_FWD, kind, {"fs": c_x}).wait_recv()

    def step_a(u, k):
        wait_in(u, k, Z_IN, c)
        when_forward(k, lambda: forward_copy(u, k).start())
        if units[u][3]:
            for copy in side_copies(u, k):
                copy.start()

    def step_b(u, k):
        to_y, to_x = corner_copies(u, k)
        wait_in(u, k, X_IN, c_x)
        to_y.start()
        wait_in(u, k, Y_IN, c_y)
        to_x.start()

    def step_c(u, k):
        wait_in(u, k, DY_IN, c_d, 0)
        wait_in(u, k, DX_IN, c_d, 1)

    for name, u in (("wq", Q), ("gv", V), ("gg", T)):
        loads[name].wait()
        send_own(u)

    loads["tok"].wait()
    values = tok_v[...].astype(F32)
    normed[...] = rms_scale(values, row_of(norm_gain)).astype(BF16)

    def rotate_lanes(v):
        half = ROPE // 2
        return (
            v * tab_v[0] + pltpu.roll(v, LANES - half, 1) * tab_v[1] + pltpu.roll(v, half, 1) * tab_v[2]
        )

    loads["lat"].wait()
    latent = rms_scale(dot(normed[...], lat_v[...]), row_of(latent_gain))
    keys[z, :, 0:KVR] = latent.astype(BF16)
    loads["rope"].wait()
    loads["tab"].wait()
    key_tmp[...] = jnp.zeros_like(key_tmp)
    key_tmp[:, 0:ROPE] = dot_nt(normed[...], rope_v[...])
    keys[z, :, KVR : KVR + LANES] = rotate_lanes(key_tmp[...]).astype(BF16)

    half_rows = rows // 2

    def key_half(shard, half):
        return keys.at[shard, pl.ds(pl.multiple_of(half * half_rows, 16), half_rows), :]

    def key_copy(shard, kind, target):
        return pltpu.make_async_remote_copy(
            src_ref=key_half(shard, t), dst_ref=key_half(shard, t),
            send_sem=key_send.at[shard, kind], recv_sem=key_recv.at[shard],
            device_id={"sp": target}, device_id_type=MESH,
        )

    def key_pair(shard, half):
        return pltpu.make_async_remote_copy(
            src_ref=key_half(shard, half), dst_ref=key_half(shard, half),
            send_sem=key_pair_send.at[shard], recv_sem=key_pair_recv.at[shard],
            device_id={"tp": peer}, device_id_type=MESH,
        )

    def own_keys(action):
        @pl.when(z > 0)
        def _():
            action(key_copy(z, Z_LOW, z - 1))

        @pl.when(z < n_sp - 1)
        def _():
            action(key_copy(z, Z_HIGH, z + 1))

    own_keys(lambda copy: copy.start())

    def step_k(k):
        shard, target = arrivals[k]
        key_copy(shard, Z_FWD, target).wait_recv()
        when_forward(k, lambda: key_copy(shard, Z_FWD, target).start())
        key_pair(shard, t).start()

    def add_shard(acc, weights, shard, first=False):
        columns = pl.ds(pl.multiple_of(shard * depth, LANES), depth)
        term = dot(normed[:, columns], weights[shard])
        acc[...] = term if first else acc[...] + term

    add_shard(q_acc, w_q, z, True)
    add_shard(v_acc, w_v, z, True)
    add_shard(t_acc, w_t, z, True)
    accs = {Q: (q_acc, w_q), V: (v_acc, w_v), T: (t_acc, w_t)}

    def step_cm(u, k):
        step_c(u, k)
        add_shard(*accs[u], arrivals[k][0])

    last = n_sp - 2
    loads["hp"].wait()
    loads["cp"].wait()
    for k in range(last + 1):
        for u in (Q, V, T):
            step_a(u, k)
            if k:
                step_b(u, k - 1)
            if k > 1:
                step_cm(u, k - 2)
        step_k(k)
        if k == 1:
            send_own(H)
    send_own(P)
    step_a(H, 0)
    for u in (Q, V, T):
        step_b(u, last)
    step_a(H, 1)
    send_own(D)
    for u in (Q, V, T):
        step_cm(u, last - 1)
    step_a(H, 2)
    step_a(P, 0)
    step_b(H, 0)
    step_cm(Q, last)

    q_lat[t] = q_acc[...]
    q_copy = pltpu.make_async_remote_copy(
        src_ref=q_lat.at[t], dst_ref=q_lat.at[t], send_sem=pair_send.at[0], recv_sem=pair_recv.at[0],
        device_id={"tp": peer}, device_id_type=MESH,
    )
    q_copy.start()
    loads["qup"].wait()
    loads["kup"].wait()
    loads["vup"].wait()
    pltpu.make_async_remote_copy(
        src_ref=q_lat.at[peer], dst_ref=q_lat.at[peer], send_sem=pair_send.at[0],
        recv_sem=pair_recv.at[0], device_id={"tp": peer}, device_id_type=MESH,
    ).wait_recv()
    whole_q = jnp.concatenate([q_lat[0], q_lat[1]], axis=1)
    latent_query = rms_scale(whole_q, row_of(query_gain)).astype(BF16)
    q_scr[...] = dot(latent_query, qup_v[...])
    for k in range(n_sp - 1):
        key_pair(arrivals[k][0], peer).wait_recv()

    def attend(h, shifted):
        start = h * (NOPE + ROPE)
        source = q_scr[...]
        if start % LANES:
            source, start = shifted, start - ROPE
        plain = source[:, start : start + NOPE].astype(BF16)
        rope_part = rotate_lanes(source[:, start + NOPE : start + NOPE + LANES]).astype(BF16)
        absorbed = dot_nt(plain, kup_v[:, h * NOPE : (h + 1) * NOPE]).astype(BF16)
        query = jnp.concatenate([absorbed, rope_part], axis=1)
        all_keys = keys[...].reshape(n_sp * rows, KVR + LANES)
        scores = dot_nt(query, all_keys) * (NOPE + ROPE) ** (-0.5)
        row_max = jnp.max(scores, axis=1, keepdims=True)
        weights = jnp.exp(scores - row_max)
        total = jnp.sum(weights, axis=1, keepdims=True)
        added = dot(weights.astype(BF16), all_keys[:, 0:KVR])
        attended = (added / total).astype(BF16)
        head_out = dot(attended, vup_v[:, h * VDIM : (h + 1) * VDIM])
        mixed[:, h * VDIM : (h + 1) * VDIM] = head_out.astype(BF16)
        return row_max + jnp.log(total)

    whole = q_scr[...]
    shifted = pltpu.roll(whole, whole.shape[1] - ROPE, 1)
    lane = lax.broadcasted_iota(jnp.int32, (rows, LANES), 1)
    logs = jnp.zeros((rows, LANES), F32)
    relays = [
        lambda: step_a(P, 1), lambda: step_b(H, 1), lambda: (step_a(D, 0), step_a(P, 2)),
        lambda: step_b(P, 0),
    ]
    for h in range(heads):
        logs = jnp.where(lane == h, attend(h, shifted), logs)
        relays[h]()
    log_out[...] = jnp.transpose(logs)[0:heads, :]

    step_cm(V, last)
    step_cm(T, last)

    halo = low_rows.shape[0]
    reach = conv_taps.shape[0] // 2
    gated[...] = (v_acc[...] * jax.nn.sigmoid(t_acc[...])).astype(BF16)
    up_copy = pltpu.make_async_remote_copy(
        src_ref=gated.at[pl.ds(rows - halo, halo), :], dst_ref=low_rows,
        send_sem=halo_send.at[0], recv_sem=halo_recv.at[0],
        device_id={"sp": z + 1}, device_id_type=MESH,
    )
    down_copy = pltpu.make_async_remote_copy(
        src_ref=gated.at[pl.ds(0, halo), :], dst_ref=high_rows,
        send_sem=halo_send.at[1], recv_sem=halo_recv.at[1],
        device_id={"sp": z - 1}, device_id_type=MESH,
    )

    @pl.when(z < n_sp - 1)
    def _():
        up_copy.start()

    @pl.when(z > 0)
    def _():
        down_copy.start()

    padded[halo : halo + rows, :] = gated[...].astype(F32)
    step_a(D, 1)
    step_b(H, 2)

    @pl.when(z > 0)
    def _():
        up_copy.wait_recv()
        padded[0:halo, :] = low_rows[...].astype(F32)

    @pl.when(z == 0)
    def _():
        padded[0:halo, :] = jnp.zeros((halo, chans), F32)

    @pl.when(z < n_sp - 1)
    def _():
        down_copy.wait_recv()
        padded[halo + rows : 2 * halo + rows, :] = high_rows[...].astype(F32)

    @pl.when(z == n_sp - 1)
    def _():
        padded[halo + rows : 2 * halo + rows, :] = jnp.zeros((halo, chans), F32)

    group = CH // GROUPS
    gains = row_of(group_gain).astype(F32)
    between = [
        lambda: step_b(P, 1), lambda: step_c(H, 0), lambda: step_a(D, 2), lambda: step_b(P, 2),
    ]
    for g in range(chans // group):
        lanes = slice(g * group, (g + 1) * group)
        taps = conv_taps[:, lanes].astype(F32)
        filtered = jnp.zeros((rows, group), F32)
        for j in range(conv_taps.shape[0]):
            first = halo - reach + j
            filtered = filtered + padded[first : first + rows, lanes] * taps[j : j + 1, :]
        centred = filtered - jnp.mean(filtered, axis=1, keepdims=True)
        spread = jnp.mean(centred * centred, axis=1, keepdims=True)
        branch = centred * lax.rsqrt(spread + norm_eps) * gains[:, lanes]
        branch = branch * jax.nn.sigmoid(branch)
        mixed[:, heads * VDIM + g * group : heads * VDIM + (g + 1) * group] = branch.astype(BF16)
        between[g]()

    def add_part(shard):
        parts[shard] = dot(mixed[...], w_o[shard]).astype(BF16)

    add_part(z)
    for k in range(n_sp - 1):
        if k:
            step_c(H, k)
        step_c(P, k)
        add_part(arrivals[k][0])

    half_sp = n_sp // 2
    p_copy = pltpu.make_async_remote_copy(
        src_ref=parts.at[pl.ds(peer * half_sp, half_sp)], dst_ref=peer_parts,
        send_sem=pair_send.at[1], recv_sem=pair_recv.at[1],
        device_id={"tp": peer}, device_id_type=MESH,
    )
    p_copy.start()

    for u in range(len(units)):
        @pl.when(z > 0)
        def _():
            own_copy(u, True).wait_send()

        @pl.when(z < n_sp - 1)
        def _():
            own_copy(u, False).wait_send()

        for k in range(n_sp - 1):
            when_forward(k, lambda: forward_copy(u, k).wait_send())
            if units[u][3]:
                for copy in side_copies(u, k) + corner_copies(u, k):
                    copy.wait_send()
    own_keys(lambda copy: copy.wait_send())
    for k in range(n_sp - 1):
        shard, target = arrivals[k]
        when_forward(k, lambda: key_copy(shard, Z_FWD, target).wait_send())
        key_pair(shard, t).wait_send()
    q_copy.wait_send()

    @pl.when(z < n_sp - 1)
    def _():
        up_copy.wait_send()

    @pl.when(z > 0)
    def _():
        down_copy.wait_send()

    p_copy.wait()
    width = parts.shape[2]
    for i in range(half_sp):
        total = parts[t * half_sp + i].astype(F32) + peer_parts[i].astype(F32)
        out[:, i * width : (i + 1) * width] = total.astype(BF16)


def fused_device(n_sp, *args):
    (tokens, norm_gain, query_down, query_gain, latent_down, latent_gain, rope_down, query_up,
     key_up, value_up, glu_value, glu_gate, conv_taps, group_gain, head_proj, channel_proj) = args
    rows, width = tokens.shape
    depth, q_rank = query_down.shape
    chans = glu_value.shape[1]
    heads = key_up.shape[1] // NOPE
    out_rows = head_proj.shape[0] + channel_proj.shape[0]
    cols = head_proj.shape[1]
    halo = (conv_taps.shape[0] // 2 + 15) // 16 * 16
    tables = jnp.asarray(rope_tables(n_sp * rows))
    vmem = pl.BlockSpec(memory_space=pltpu.VMEM)
    hbm = pl.BlockSpec(memory_space=pltpu.HBM)
    as_row = lambda v: v
    operands = [
        (tokens, hbm), (as_row(norm_gain), vmem), (query_down, hbm), (as_row(query_gain), vmem),
        (latent_down, hbm), (as_row(latent_gain), vmem), (rope_down.T, hbm), (query_up, hbm),
        (key_up, hbm), (value_up, hbm), (glu_value, hbm), (glu_gate, hbm), (conv_taps, vmem),
        (as_row(group_gain), vmem), (head_proj, hbm), (channel_proj, hbm), (tables, hbm),
    ]
    like = lambda a: pltpu.VMEM(a.shape, a.dtype)
    dma = pltpu.SemaphoreType.DMA
    scratch = [
        pltpu.VMEM((n_sp, depth, q_rank // 2), BF16),
        pltpu.VMEM((n_sp, depth, chans), BF16),
        pltpu.VMEM((n_sp, depth, chans), BF16),
        pltpu.VMEM((n_sp, out_rows, cols), BF16),
        like(tokens), like(latent_down), pltpu.VMEM(rope_down.shape[::-1], BF16), like(query_up), like(key_up), like(value_up),
        pltpu.VMEM((3, rows, LANES), F32),
        pltpu.VMEM((rows, width), BF16),
        pltpu.VMEM((n_sp, rows, KVR + LANES), BF16),
        pltpu.VMEM((rows, LANES), F32),
        pltpu.VMEM((rows, q_rank // 2), F32),
        pltpu.VMEM((2, rows, q_rank // 2), F32),
        pltpu.VMEM((rows, query_up.shape[1]), F32),
        pltpu.VMEM((rows, chans), F32),
        pltpu.VMEM((rows, chans), F32),
        pltpu.VMEM((rows, out_rows), BF16),
        pltpu.VMEM((rows, chans), BF16),
        pltpu.VMEM((halo, chans), BF16),
        pltpu.VMEM((halo, chans), BF16),
        pltpu.VMEM((rows + 2 * halo, chans), F32),
        pltpu.VMEM((n_sp, rows, cols), BF16),
        pltpu.VMEM((n_sp // 2, rows, cols), BF16),
        dma((12,)), dma((6, n_sp, 5)), dma((6, n_sp, 7)), dma((n_sp,)), dma((n_sp, 3)), dma((n_sp,)),
        dma((n_sp,)),
        dma((2,)), dma((2,)), dma((2,)), dma((2,)),
    ]
    return pl.pallas_call(
        functools.partial(fused_kernel, n_sp),
        out_shape=(
            jax.ShapeDtypeStruct((rows, n_sp * cols // 2), BF16),
            jax.ShapeDtypeStruct((heads, rows), F32),
        ),
        in_specs=[spec for _, spec in operands],
        out_specs=(vmem, vmem),
        scratch_shapes=scratch,
        compiler_params=pltpu.CompilerParams(
            collective_id=0, has_side_effects=True, vmem_limit_bytes=63 * 1024 * 1024
        ),
        name="fused_layer",
    )(*[value for value, _ in operands])


def solution(mesh):
    in_specs = (
        P(("fs", "sp"), None),
        P(),
        P("sp", None),
        P(),
        P(),
        P(),
        P(),
        P(None, "tp"),
        P(None, "tp"),
        P(None, "tp"),
        P("sp", "tp"),
        P("sp", "tp"),
        P(None, "tp"),
        P("tp"),
        P("tp", "sp"),
        P("tp", "sp"),
    )
    out_specs = (P(("fs", "sp"), "tp"), P("tp", ("fs", "sp")))
    body = per_device
    if mesh.shape["fs"] == 4 and mesh.shape["tp"] == 2 and mesh.shape["sp"] == 4:
        body = functools.partial(fused_device, mesh.shape["sp"])
    return jax.shard_map(
        body, mesh=mesh, in_specs=in_specs, out_specs=out_specs, check_vma=False
    )
```

```python
import functools

import jax
import jax.numpy as jnp
import numpy as np
from jax import lax
from jax.experimental import pallas as pl
from jax.experimental.pallas import tpu as pltpu
from jax.sharding import PartitionSpec as P

NOPE = 128
ROPE = 64
VDIM = 128
KVR = 256
CH = 1024
GROUPS = 8
GRID_W = 64


norm_eps = 1e-06
rope_base = 10000.0
far_below = -1e30


def padded_2(block, sides, width):
    for axis, dim in sides:
        count = lax.axis_size(axis)
        forward = [(i, i + 1) for i in range(count - 1)]
        backward = [(target, source) for source, target in forward]
        low = lax.ppermute(
            lax.slice_in_dim(block, block.shape[dim] - width, None, axis=dim), axis, forward
        )
        high = lax.ppermute(lax.slice_in_dim(block, 0, width, axis=dim), axis, backward)
        block = jnp.concatenate([low, block, high], axis=dim)
    return block


def rms_scale(values, scale_gain):
    inv_rms = lax.rsqrt(jnp.mean(values * values, axis=-1, keepdims=True) + norm_eps)
    return values * inv_rms * scale_gain.astype(jnp.float32)


def angles_for(positions, rope_size):
    quarter = rope_size // 4
    inverse = rope_base ** (-jnp.arange(quarter, dtype=jnp.float32) / quarter)
    grid_row = (positions // GRID_W).astype(jnp.float32)
    grid_col = (positions % GRID_W).astype(jnp.float32)
    return jnp.concatenate([grid_row[:, None] * inverse, grid_col[:, None] * inverse], axis=-1)


def rotate(values, angles):
    half_size = values.shape[-1] // 2
    front_half = values[..., :half_size]
    back_half = values[..., half_size:]
    cosine = jnp.cos(angles)
    sine_part = jnp.sin(angles)
    return jnp.concatenate(
        [front_half * cosine - back_half * sine_part, back_half * cosine + front_half * sine_part],
        axis=-1,
    )


def key_block(normed, latent_down, latent_gain, rope_down, positions):
    latent = jnp.dot(normed, latent_down, preferred_element_type=jnp.float32)
    latent = rms_scale(latent, latent_gain).astype(jnp.bfloat16)
    rope_key = jnp.dot(normed, rope_down, preferred_element_type=jnp.float32)
    rope_key = rotate(rope_key, angles_for(positions, rope_key.shape[-1])).astype(jnp.bfloat16)
    return jnp.concatenate([latent, rope_key], axis=1)


def per_device(
    tokens,
    norm_gain,
    query_down,
    query_gain,
    latent_down,
    latent_gain,
    rope_down,
    query_up,
    key_up,
    value_up,
    glu_value,
    glu_gate,
    conv_taps,
    group_gain,
    head_proj,
    channel_proj,
):
    tok_count = tokens.shape[0]
    reach_rows = conv_taps.shape[0] // 2
    head_count = key_up.shape[1] // NOPE
    normed = rms_scale(tokens.astype(jnp.float32), norm_gain).astype(jnp.bfloat16)
    offsets = lax.axis_index("sp") * tok_count + jnp.arange(tok_count, dtype=jnp.int32)
    query_latent = jnp.dot(
        normed,
        lax.all_gather(query_down, "sp", axis=0, tiled=True),
        preferred_element_type=jnp.float32,
    )
    value_in = jnp.dot(
        normed,
        lax.all_gather(glu_value, "sp", axis=0, tiled=True),
        preferred_element_type=jnp.float32,
    )
    gate_in = jnp.dot(
        normed,
        lax.all_gather(glu_gate, "sp", axis=0, tiled=True),
        preferred_element_type=jnp.float32,
    )
    latent_query = rms_scale(query_latent, query_gain).astype(jnp.bfloat16)
    query_all = jnp.dot(latent_query, query_up, preferred_element_type=jnp.float32).reshape(
        tok_count, head_count, NOPE + ROPE
    )
    query_plain = query_all[:, :, :NOPE].astype(jnp.bfloat16)
    query_rope = rotate(query_all[:, :, NOPE:], angles_for(offsets, ROPE)[:, None, :]).astype(
        jnp.bfloat16
    )
    absorbed = jnp.einsum(
        "thd,rhd->htr",
        query_plain,
        key_up.reshape(KVR, head_count, NOPE),
        preferred_element_type=jnp.float32,
    ).astype(jnp.bfloat16)
    queries = jnp.concatenate([absorbed, jnp.transpose(query_rope, (1, 0, 2))], axis=-1)
    score_scale = (NOPE + ROPE) ** (-0.5)
    half_rows = tok_count // lax.axis_size("tp")
    first_row = lax.axis_index("tp") * half_rows
    own_rows = lax.dynamic_slice_in_dim(normed, first_row, half_rows, 0)
    own_positions = lax.dynamic_slice_in_dim(offsets, first_row, half_rows, 0)
    own_keys = key_block(own_rows, latent_down, latent_gain, rope_down, own_positions)
    block_keys = lax.all_gather(own_keys, ("sp", "tp"), axis=0, tiled=True)
    row_max = jnp.full((head_count, tok_count), far_below, jnp.float32)
    scores = (
        jnp.einsum("hqc,kc->hqk", queries, block_keys, preferred_element_type=jnp.float32)
        * score_scale
    )
    new_max = jnp.maximum(row_max, jnp.max(scores, axis=2))
    weights = jnp.exp(scores - new_max[:, :, None])
    new_sum = jnp.sum(weights, axis=2)
    added = jnp.einsum(
        "hqk,kr->hqr",
        weights.astype(jnp.bfloat16),
        block_keys[:, :KVR],
        preferred_element_type=jnp.float32,
    )
    gated_rows = (value_in * jax.nn.sigmoid(gate_in)).astype(jnp.bfloat16)
    padded = padded_2(gated_rows, (("sp", 0),), reach_rows)
    filtered = padded[0:tok_count].astype(jnp.float32) * conv_taps[0].astype(jnp.float32)
    for tap_index in range(1, conv_taps.shape[0]):
        filtered = filtered + padded[tap_index : tap_index + tok_count].astype(
            jnp.float32
        ) * conv_taps[tap_index].astype(jnp.float32)
    grouped = filtered.reshape(tok_count, -1, CH // GROUPS)
    centred = grouped - jnp.mean(grouped, axis=-1, keepdims=True)
    spread = jnp.mean(centred * centred, axis=-1, keepdims=True)
    normal_groups = (centred * lax.rsqrt(spread + norm_eps)).reshape(tok_count, -1)
    conv_branch = jax.nn.silu(normal_groups * group_gain.astype(jnp.float32)).astype(jnp.bfloat16)
    attended = (added / new_sum[:, :, None]).astype(jnp.bfloat16)
    log_weight = new_max + jnp.log(new_sum)
    head_out = jnp.einsum(
        "htr,rhv->thv",
        attended,
        value_up.reshape(KVR, head_count, VDIM),
        preferred_element_type=jnp.float32,
    )
    head_out = head_out.reshape(tok_count, head_count * VDIM).astype(jnp.bfloat16)
    mixed_in = jnp.concatenate([head_out, conv_branch], axis=1)
    out_weight = jnp.concatenate([head_proj, channel_proj], axis=0)
    partial_terms = jnp.dot(
        mixed_in,
        lax.all_gather(out_weight, "sp", axis=1, tiled=True),
        preferred_element_type=jnp.float32,
    )
    mixed_out = lax.psum_scatter(
        partial_terms.astype(jnp.bfloat16), "tp", scatter_dimension=1, tiled=True
    )
    return (mixed_out, log_weight)


LANES = 128
MESH = pl.DeviceIdType.MESH
F32 = jnp.float32
BF16 = jnp.bfloat16
Z_IN, X_IN, Y_IN, DX_IN, DY_IN = range(5)
Z_LOW, Z_HIGH, Z_FWD, X_OUT, Y_OUT, DX_OUT, DY_OUT = range(7)


def rope_tables(length):
    quarter = ROPE // 4
    inverse = np.float32(rope_base) ** (-np.arange(quarter, dtype=np.float32) / np.float32(quarter))
    positions = np.arange(length)
    row = (positions // GRID_W).astype(np.float32)[:, None] * inverse
    col = (positions % GRID_W).astype(np.float32)[:, None] * inverse
    angles = np.concatenate([row, col], axis=1).astype(np.float32)
    cosine, sine = np.cos(angles), np.sin(angles)
    tables = np.zeros((3, length, LANES), np.float32)
    half = ROPE // 2
    tables[0, :, :half] = cosine
    tables[0, :, half:ROPE] = cosine
    tables[1, :, :half] = -sine
    tables[2, :, half:ROPE] = sine
    return tables


def dot(a, b):
    return jnp.dot(a, b, preferred_element_type=F32)


def row_of(ref):
    return ref[...].reshape(1, -1)


def dot_nt(a, b):
    return lax.dot_general(a, b, (((1,), (1,)), ((), ())), preferred_element_type=F32)


def fused_kernel(
    n_sp,
    tokens, norm_gain, query_down, query_gain, latent_down, latent_gain, rope_down, query_up,
    key_up, value_up, glu_value, glu_gate, conv_taps, group_gain, head_proj, channel_proj, tables,
    out, log_out,
    w_q, w_v, w_t, w_o, tok_v, lat_v, rope_v, qup_v, kup_v, vup_v, tab_v,
    normed, keys, key_tmp, q_acc, q_lat, q_scr, v_acc, t_acc, mixed, gated, low_rows, high_rows, padded,
    parts, peer_parts,
    load_sem, recv_sem, send_sem, key_recv, key_send, key_pair_recv, key_pair_send, pair_recv, pair_send, halo_recv, halo_send,
):
    z = lax.axis_index("sp")
    c = lax.axis_index("fs")
    t = lax.axis_index("tp")
    peer = 1 - t
    c_x = c + 1 - 2 * (c % 2)
    c_y = (c + 2) % 4
    c_d = 3 - c
    rows = tokens.shape[0]
    depth = query_down.shape[0]
    q_cols = w_q.shape[2]
    chans = glu_value.shape[1]
    heads = key_up.shape[1] // NOPE
    head_rows = head_proj.shape[0]
    out_rows = w_o.shape[1]

    loads = {}

    def load(name, src, dst):
        copy = pltpu.make_async_copy(src, dst, load_sem.at[len(loads)])
        copy.start()
        loads[name] = copy

    load("wq", query_down.at[:, pl.ds(pl.multiple_of(t * q_cols, LANES), q_cols)], w_q.at[z])
    load("gv", glu_value, w_v.at[z])
    load("gg", glu_gate, w_t.at[z])
    load("tok", tokens, tok_v)
    load("lat", latent_down, lat_v)
    load("rope", rope_down, rope_v)
    load("tab", tables.at[:, pl.ds(pl.multiple_of(z * rows, LANES), rows), :], tab_v)
    load("hp", head_proj, w_o.at[z, pl.ds(0, head_rows), :])
    load("cp", channel_proj, w_o.at[z, pl.ds(head_rows, out_rows - head_rows), :])
    load("qup", query_up, qup_v)
    load("kup", key_up, kup_v)
    load("vup", value_up, vup_v)

    barrier = pltpu.get_barrier_semaphore()
    sides = [{"fs": c_x}, {"fs": c_y}, {"tp": peer}]
    for partner in sides:
        pl.semaphore_signal(barrier, inc=1, device_id=partner, device_id_type=MESH)

    @pl.when(z > 0)
    def _():
        pl.semaphore_signal(barrier, inc=1, device_id={"sp": z - 1}, device_id_type=MESH)

    @pl.when(z < n_sp - 1)
    def _():
        pl.semaphore_signal(barrier, inc=1, device_id={"sp": z + 1}, device_id_type=MESH)

    ends = (z == 0).astype(jnp.int32) + (z == n_sp - 1).astype(jnp.int32)
    pl.semaphore_wait(barrier, len(sides) + 2 - ends)

    direct_rows = (out_rows // 8) // 64 * 64
    units = [
        (w_q, 0, depth, True),
        (w_v, 0, depth, True),
        (w_t, 0, depth, True),
        (w_o, 0, head_rows, True),
        (w_o, head_rows, out_rows - head_rows - direct_rows, True),
        (w_o, out_rows - direct_rows, direct_rows, False),
    ]
    Q, V, T, H, P, D = range(6)

    def block(u, shard, quarter, half=None):
        buf, first, count, shared = units[u]
        if not shared:
            return buf.at[shard, pl.ds(first, count), :]
        size = count // 4
        start = first + quarter * size
        if half is not None:
            size = size // 2
            start = start + half * size
        return buf.at[shard, pl.ds(pl.multiple_of(start, 16), size), :]

    def remote(u, shard, ref, out_kind, in_kind, device):
        return pltpu.make_async_remote_copy(
            src_ref=ref, dst_ref=ref,
            send_sem=send_sem.at[u, shard, out_kind], recv_sem=recv_sem.at[u, shard, in_kind],
            device_id=device, device_id_type=MESH,
        )

    def own_copy(u, low):
        return remote(
            u, z, block(u, z, c), Z_LOW if low else Z_HIGH, Z_IN, {"sp": z - 1 if low else z + 1}
        )

    def send_own(u):
        @pl.when(z > 0)
        def _():
            own_copy(u, True).start()

        @pl.when(z < n_sp - 1)
        def _():
            own_copy(u, False).start()

    nearest = jnp.minimum(z, n_sp - 1 - z)
    arrivals = []
    for k in range(n_sp - 1):
        both = k < 2 * nearest
        distance = jnp.where(both, k // 2 + 1, k - nearest + 1)
        from_low = jnp.where(both, 1 - k % 2, (2 * z > n_sp - 1).astype(jnp.int32))
        shard = z - distance * (2 * from_low - 1)
        arrivals.append((shard, z + 2 * from_low - 1))

    def forward_copy(u, k):
        shard, target = arrivals[k]
        return remote(u, shard, block(u, shard, c), Z_FWD, Z_IN, {"sp": target})

    def when_forward(k, action):
        target = arrivals[k][1]

        @pl.when((target >= 0) & (target < n_sp))
        def _():
            action()

    def side_copies(u, k):
        shard, _ = arrivals[k]
        mine = block(u, shard, c)
        return (
            remote(u, shard, mine, X_OUT, X_IN, {"fs": c_x}),
            remote(u, shard, mine, Y_OUT, Y_IN, {"fs": c_y}),
        )

    def corner_copies(u, k):
        shard, _ = arrivals[k]
        return (
            remote(u, shard, block(u, shard, c_x, 0), DY_OUT, DY_IN, {"fs": c_y}),
            remote(u, shard, block(u, shard, c_y, 1), DX_OUT, DX_IN, {"fs": c_x}),
        )

    def wait_in(u, k, kind, quarter, half=None):
        shard, _ = arrivals[k]
        remote(u, shard, block(u, shard, quarter, half), Z_FWD, kind, {"fs": c_x}).wait_recv()

    def step_a(u, k):
        wait_in(u, k, Z_IN, c)
        when_forward(k, lambda: forward_copy(u, k).start())
        if units[u][3]:
            for copy in side_copies(u, k):
                copy.start()

    def step_b(u, k):
        to_y, to_x = corner_copies(u, k)
        wait_in(u, k, X_IN, c_x)
        to_y.start()
        wait_in(u, k, Y_IN, c_y)
        to_x.start()

    def step_c(u, k):
        wait_in(u, k, DY_IN, c_d, 0)
        wait_in(u, k, DX_IN, c_d, 1)

    for name, u in (("wq", Q), ("gv", V), ("gg", T)):
        loads[name].wait()
        send_own(u)

    loads["tok"].wait()
    values = tok_v[...].astype(F32)
    normed[...] = rms_scale(values, row_of(norm_gain)).astype(BF16)

    def rotate_lanes(v):
        half = ROPE // 2
        return (
            v * tab_v[0] + pltpu.roll(v, LANES - half, 1) * tab_v[1] + pltpu.roll(v, half, 1) * tab_v[2]
        )

    loads["lat"].wait()
    latent = rms_scale(dot(normed[...], lat_v[...]), row_of(latent_gain))
    keys[z, :, 0:KVR] = latent.astype(BF16)
    loads["rope"].wait()
    loads["tab"].wait()
    key_tmp[...] = jnp.zeros_like(key_tmp)
    key_tmp[:, 0:ROPE] = dot_nt(normed[...], rope_v[...])
    keys[z, :, KVR : KVR + LANES] = rotate_lanes(key_tmp[...]).astype(BF16)

    half_rows = rows // 2

    def key_half(shard, half):
        return keys.at[shard, pl.ds(pl.multiple_of(half * half_rows, 16), half_rows), :]

    def key_copy(shard, kind, target):
        return pltpu.make_async_remote_copy(
            src_ref=key_half(shard, t), dst_ref=key_half(shard, t),
            send_sem=key_send.at[shard, kind], recv_sem=key_recv.at[shard],
            device_id={"sp": target}, device_id_type=MESH,
        )

    def key_pair(shard, half):
        return pltpu.make_async_remote_copy(
            src_ref=key_half(shard, half), dst_ref=key_half(shard, half),
            send_sem=key_pair_send.at[shard], recv_sem=key_pair_recv.at[shard],
            device_id={"tp": peer}, device_id_type=MESH,
        )

    def own_keys(action):
        @pl.when(z > 0)
        def _():
            action(key_copy(z, Z_LOW, z - 1))

        @pl.when(z < n_sp - 1)
        def _():
            action(key_copy(z, Z_HIGH, z + 1))

    own_keys(lambda copy: copy.start())

    def step_k(k):
        shard, target = arrivals[k]
        key_copy(shard, Z_FWD, target).wait_recv()
        when_forward(k, lambda: key_copy(shard, Z_FWD, target).start())
        key_pair(shard, t).start()

    def add_shard(acc, weights, shard, first=False):
        columns = pl.ds(pl.multiple_of(shard * depth, LANES), depth)
        term = dot(normed[:, columns], weights[shard])
        acc[...] = term if first else acc[...] + term

    add_shard(q_acc, w_q, z, True)
    add_shard(v_acc, w_v, z, True)
    add_shard(t_acc, w_t, z, True)
    accs = {Q: (q_acc, w_q), V: (v_acc, w_v), T: (t_acc, w_t)}

    def step_cm(u, k):
        step_c(u, k)
        add_shard(*accs[u], arrivals[k][0])

    last = n_sp - 2
    loads["hp"].wait()
    loads["cp"].wait()
    for k in range(last + 1):
        for u in (Q, V, T):
            step_a(u, k)
            if k:
                step_b(u, k - 1)
            if k > 1:
                step_cm(u, k - 2)
        step_k(k)
        if k == 1:
            send_own(H)
    send_own(P)
    step_b(Q, last)
    step_a(H, 0)
    step_b(V, last)
    step_a(H, 1)
    step_b(T, last)
    send_own(D)
    for u in (Q, V, T):
        step_cm(u, last - 1)
    step_b(H, 0)
    step_a(P, 0)
    step_cm(Q, last)
    step_a(H, 2)

    q_lat[t] = q_acc[...]
    q_copy = pltpu.make_async_remote_copy(
        src_ref=q_lat.at[t], dst_ref=q_lat.at[t], send_sem=pair_send.at[0], recv_sem=pair_recv.at[0],
        device_id={"tp": peer}, device_id_type=MESH,
    )
    q_copy.start()
    loads["qup"].wait()
    loads["kup"].wait()
    loads["vup"].wait()
    pltpu.make_async_remote_copy(
        src_ref=q_lat.at[peer], dst_ref=q_lat.at[peer], send_sem=pair_send.at[0],
        recv_sem=pair_recv.at[0], device_id={"tp": peer}, device_id_type=MESH,
    ).wait_recv()
    whole_q = jnp.concatenate([q_lat[0], q_lat[1]], axis=1)
    latent_query = rms_scale(whole_q, row_of(query_gain)).astype(BF16)
    q_scr[...] = dot(latent_query, qup_v[...])
    for k in range(n_sp - 1):
        key_pair(arrivals[k][0], peer).wait_recv()

    def attend(h, shifted):
        start = h * (NOPE + ROPE)
        source = q_scr[...]
        if start % LANES:
            source, start = shifted, start - ROPE
        plain = source[:, start : start + NOPE].astype(BF16)
        rope_part = rotate_lanes(source[:, start + NOPE : start + NOPE + LANES]).astype(BF16)
        absorbed = dot_nt(plain, kup_v[:, h * NOPE : (h + 1) * NOPE]).astype(BF16)
        query = jnp.concatenate([absorbed, rope_part], axis=1)
        all_keys = keys[...].reshape(n_sp * rows, KVR + LANES)
        scores = dot_nt(query, all_keys) * (NOPE + ROPE) ** (-0.5)
        row_max = jnp.max(scores, axis=1, keepdims=True)
        weights = jnp.exp(scores - row_max)
        total = jnp.sum(weights, axis=1, keepdims=True)
        added = dot(weights.astype(BF16), all_keys[:, 0:KVR])
        attended = (added / total).astype(BF16)
        head_out = dot(attended, vup_v[:, h * VDIM : (h + 1) * VDIM])
        mixed[:, h * VDIM : (h + 1) * VDIM] = head_out.astype(BF16)
        return row_max + jnp.log(total)

    whole = q_scr[...]
    shifted = pltpu.roll(whole, whole.shape[1] - ROPE, 1)
    lane = lax.broadcasted_iota(jnp.int32, (rows, LANES), 1)
    logs = jnp.zeros((rows, LANES), F32)
    relays = [
        lambda: step_a(P, 1), lambda: step_b(H, 1), lambda: (step_a(D, 0), step_a(P, 2)),
        lambda: step_b(P, 0),
    ]
    for h in range(heads):
        logs = jnp.where(lane == h, attend(h, shifted), logs)
        relays[h]()
    log_out[...] = jnp.transpose(logs)[0:heads, :]

    step_cm(V, last)
    step_cm(T, last)

    halo = low_rows.shape[0]
    reach = conv_taps.shape[0] // 2
    gated[...] = (v_acc[...] * jax.nn.sigmoid(t_acc[...])).astype(BF16)
    up_copy = pltpu.make_async_remote_copy(
        src_ref=gated.at[pl.ds(rows - halo, halo), :], dst_ref=low_rows,
        send_sem=halo_send.at[0], recv_sem=halo_recv.at[0],
        device_id={"sp": z + 1}, device_id_type=MESH,
    )
    down_copy = pltpu.make_async_remote_copy(
        src_ref=gated.at[pl.ds(0, halo), :], dst_ref=high_rows,
        send_sem=halo_send.at[1], recv_sem=halo_recv.at[1],
        device_id={"sp": z - 1}, device_id_type=MESH,
    )

    @pl.when(z < n_sp - 1)
    def _():
        up_copy.start()

    @pl.when(z > 0)
    def _():
        down_copy.start()

    padded[halo : halo + rows, :] = gated[...].astype(F32)
    step_a(D, 1)
    step_b(H, 2)

    @pl.when(z > 0)
    def _():
        up_copy.wait_recv()
        padded[0:halo, :] = low_rows[...].astype(F32)

    @pl.when(z == 0)
    def _():
        padded[0:halo, :] = jnp.zeros((halo, chans), F32)

    @pl.when(z < n_sp - 1)
    def _():
        down_copy.wait_recv()
        padded[halo + rows : 2 * halo + rows, :] = high_rows[...].astype(F32)

    @pl.when(z == n_sp - 1)
    def _():
        padded[halo + rows : 2 * halo + rows, :] = jnp.zeros((halo, chans), F32)

    group = CH // GROUPS
    gains = row_of(group_gain).astype(F32)
    between = [
        lambda: step_b(P, 1), lambda: step_c(H, 0), lambda: step_a(D, 2), lambda: step_b(P, 2),
    ]
    for g in range(chans // group):
        lanes = slice(g * group, (g + 1) * group)
        taps = conv_taps[:, lanes].astype(F32)
        filtered = jnp.zeros((rows, group), F32)
        for j in range(conv_taps.shape[0]):
            first = halo - reach + j
            filtered = filtered + padded[first : first + rows, lanes] * taps[j : j + 1, :]
        centred = filtered - jnp.mean(filtered, axis=1, keepdims=True)
        spread = jnp.mean(centred * centred, axis=1, keepdims=True)
        branch = centred * lax.rsqrt(spread + norm_eps) * gains[:, lanes]
        branch = branch * jax.nn.sigmoid(branch)
        mixed[:, heads * VDIM + g * group : heads * VDIM + (g + 1) * group] = branch.astype(BF16)
        between[g]()

    def add_part(shard):
        parts[shard] = dot(mixed[...], w_o[shard]).astype(BF16)

    add_part(z)
    for k in range(n_sp - 1):
        if k:
            step_c(H, k)
        step_c(P, k)
        add_part(arrivals[k][0])

    half_sp = n_sp // 2
    p_copy = pltpu.make_async_remote_copy(
        src_ref=parts.at[pl.ds(peer * half_sp, half_sp)], dst_ref=peer_parts,
        send_sem=pair_send.at[1], recv_sem=pair_recv.at[1],
        device_id={"tp": peer}, device_id_type=MESH,
    )
    p_copy.start()

    for u in range(len(units)):
        @pl.when(z > 0)
        def _():
            own_copy(u, True).wait_send()

        @pl.when(z < n_sp - 1)
        def _():
            own_copy(u, False).wait_send()

        for k in range(n_sp - 1):
            when_forward(k, lambda: forward_copy(u, k).wait_send())
            if units[u][3]:
                for copy in side_copies(u, k) + corner_copies(u, k):
                    copy.wait_send()
    own_keys(lambda copy: copy.wait_send())
    for k in range(n_sp - 1):
        shard, target = arrivals[k]
        when_forward(k, lambda: key_copy(shard, Z_FWD, target).wait_send())
        key_pair(shard, t).wait_send()
    q_copy.wait_send()

    @pl.when(z < n_sp - 1)
    def _():
        up_copy.wait_send()

    @pl.when(z > 0)
    def _():
        down_copy.wait_send()

    p_copy.wait()
    width = parts.shape[2]
    for i in range(half_sp):
        total = parts[t * half_sp + i].astype(F32) + peer_parts[i].astype(F32)
        out[:, i * width : (i + 1) * width] = total.astype(BF16)


def fused_device(n_sp, *args):
    (tokens, norm_gain, query_down, query_gain, latent_down, latent_gain, rope_down, query_up,
     key_up, value_up, glu_value, glu_gate, conv_taps, group_gain, head_proj, channel_proj) = args
    rows, width = tokens.shape
    depth, q_rank = query_down.shape
    chans = glu_value.shape[1]
    heads = key_up.shape[1] // NOPE
    out_rows = head_proj.shape[0] + channel_proj.shape[0]
    cols = head_proj.shape[1]
    halo = (conv_taps.shape[0] // 2 + 15) // 16 * 16
    tables = jnp.asarray(rope_tables(n_sp * rows))
    vmem = pl.BlockSpec(memory_space=pltpu.VMEM)
    hbm = pl.BlockSpec(memory_space=pltpu.HBM)
    as_row = lambda v: v
    operands = [
        (tokens, hbm), (as_row(norm_gain), vmem), (query_down, hbm), (as_row(query_gain), vmem),
        (latent_down, hbm), (as_row(latent_gain), vmem), (rope_down.T, hbm), (query_up, hbm),
        (key_up, hbm), (value_up, hbm), (glu_value, hbm), (glu_gate, hbm), (conv_taps, vmem),
        (as_row(group_gain), vmem), (head_proj, hbm), (channel_proj, hbm), (tables, hbm),
    ]
    like = lambda a: pltpu.VMEM(a.shape, a.dtype)
    dma = pltpu.SemaphoreType.DMA
    scratch = [
        pltpu.VMEM((n_sp, depth, q_rank // 2), BF16),
        pltpu.VMEM((n_sp, depth, chans), BF16),
        pltpu.VMEM((n_sp, depth, chans), BF16),
        pltpu.VMEM((n_sp, out_rows, cols), BF16),
        like(tokens), like(latent_down), pltpu.VMEM(rope_down.shape[::-1], BF16), like(query_up), like(key_up), like(value_up),
        pltpu.VMEM((3, rows, LANES), F32),
        pltpu.VMEM((rows, width), BF16),
        pltpu.VMEM((n_sp, rows, KVR + LANES), BF16),
        pltpu.VMEM((rows, LANES), F32),
        pltpu.VMEM((rows, q_rank // 2), F32),
        pltpu.VMEM((2, rows, q_rank // 2), F32),
        pltpu.VMEM((rows, query_up.shape[1]), F32),
        pltpu.VMEM((rows, chans), F32),
        pltpu.VMEM((rows, chans), F32),
        pltpu.VMEM((rows, out_rows), BF16),
        pltpu.VMEM((rows, chans), BF16),
        pltpu.VMEM((halo, chans), BF16),
        pltpu.VMEM((halo, chans), BF16),
        pltpu.VMEM((rows + 2 * halo, chans), F32),
        pltpu.VMEM((n_sp, rows, cols), BF16),
        pltpu.VMEM((n_sp // 2, rows, cols), BF16),
        dma((12,)), dma((6, n_sp, 5)), dma((6, n_sp, 7)), dma((n_sp,)), dma((n_sp, 3)), dma((n_sp,)),
        dma((n_sp,)),
        dma((2,)), dma((2,)), dma((2,)), dma((2,)),
    ]
    return pl.pallas_call(
        functools.partial(fused_kernel, n_sp),
        out_shape=(
            jax.ShapeDtypeStruct((rows, n_sp * cols // 2), BF16),
            jax.ShapeDtypeStruct((heads, rows), F32),
        ),
        in_specs=[spec for _, spec in operands],
        out_specs=(vmem, vmem),
        scratch_shapes=scratch,
        compiler_params=pltpu.CompilerParams(
            collective_id=0, has_side_effects=True, vmem_limit_bytes=63 * 1024 * 1024
        ),
        name="fused_layer",
    )(*[value for value, _ in operands])


def solution(mesh):
    in_specs = (
        P(("fs", "sp"), None),
        P(),
        P("sp", None),
        P(),
        P(),
        P(),
        P(),
        P(None, "tp"),
        P(None, "tp"),
        P(None, "tp"),
        P("sp", "tp"),
        P("sp", "tp"),
        P(None, "tp"),
        P("tp"),
        P("tp", "sp"),
        P("tp", "sp"),
    )
    out_specs = (P(("fs", "sp"), "tp"), P("tp", ("fs", "sp")))
    body = per_device
    if mesh.shape["fs"] == 4 and mesh.shape["tp"] == 2 and mesh.shape["sp"] == 4:
        body = functools.partial(fused_device, mesh.shape["sp"])
    return jax.shard_map(
        body, mesh=mesh, in_specs=in_specs, out_specs=out_specs, check_vma=False
    )
```

```python
import functools

import jax
import jax.numpy as jnp
import numpy as np
from jax import lax
from jax.experimental import pallas as pl
from jax.experimental.pallas import tpu as pltpu
from jax.sharding import PartitionSpec as P

NOPE = 128
ROPE = 64
VDIM = 128
KVR = 256
CH = 1024
GROUPS = 8
GRID_W = 64


norm_eps = 1e-06
rope_base = 10000.0
far_below = -1e30


def padded_2(block, sides, width):
    for axis, dim in sides:
        count = lax.axis_size(axis)
        forward = [(i, i + 1) for i in range(count - 1)]
        backward = [(target, source) for source, target in forward]
        low = lax.ppermute(
            lax.slice_in_dim(block, block.shape[dim] - width, None, axis=dim), axis, forward
        )
        high = lax.ppermute(lax.slice_in_dim(block, 0, width, axis=dim), axis, backward)
        block = jnp.concatenate([low, block, high], axis=dim)
    return block


def rms_scale(values, scale_gain):
    inv_rms = lax.rsqrt(jnp.mean(values * values, axis=-1, keepdims=True) + norm_eps)
    return values * inv_rms * scale_gain.astype(jnp.float32)


def angles_for(positions, rope_size):
    quarter = rope_size // 4
    inverse = rope_base ** (-jnp.arange(quarter, dtype=jnp.float32) / quarter)
    grid_row = (positions // GRID_W).astype(jnp.float32)
    grid_col = (positions % GRID_W).astype(jnp.float32)
    return jnp.concatenate([grid_row[:, None] * inverse, grid_col[:, None] * inverse], axis=-1)


def rotate(values, angles):
    half_size = values.shape[-1] // 2
    front_half = values[..., :half_size]
    back_half = values[..., half_size:]
    cosine = jnp.cos(angles)
    sine_part = jnp.sin(angles)
    return jnp.concatenate(
        [front_half * cosine - back_half * sine_part, back_half * cosine + front_half * sine_part],
        axis=-1,
    )


def key_block(normed, latent_down, latent_gain, rope_down, positions):
    latent = jnp.dot(normed, latent_down, preferred_element_type=jnp.float32)
    latent = rms_scale(latent, latent_gain).astype(jnp.bfloat16)
    rope_key = jnp.dot(normed, rope_down, preferred_element_type=jnp.float32)
    rope_key = rotate(rope_key, angles_for(positions, rope_key.shape[-1])).astype(jnp.bfloat16)
    return jnp.concatenate([latent, rope_key], axis=1)


def per_device(
    tokens,
    norm_gain,
    query_down,
    query_gain,
    latent_down,
    latent_gain,
    rope_down,
    query_up,
    key_up,
    value_up,
    glu_value,
    glu_gate,
    conv_taps,
    group_gain,
    head_proj,
    channel_proj,
):
    tok_count = tokens.shape[0]
    reach_rows = conv_taps.shape[0] // 2
    head_count = key_up.shape[1] // NOPE
    normed = rms_scale(tokens.astype(jnp.float32), norm_gain).astype(jnp.bfloat16)
    offsets = lax.axis_index("sp") * tok_count + jnp.arange(tok_count, dtype=jnp.int32)
    query_latent = jnp.dot(
        normed,
        lax.all_gather(query_down, "sp", axis=0, tiled=True),
        preferred_element_type=jnp.float32,
    )
    value_in = jnp.dot(
        normed,
        lax.all_gather(glu_value, "sp", axis=0, tiled=True),
        preferred_element_type=jnp.float32,
    )
    gate_in = jnp.dot(
        normed,
        lax.all_gather(glu_gate, "sp", axis=0, tiled=True),
        preferred_element_type=jnp.float32,
    )
    latent_query = rms_scale(query_latent, query_gain).astype(jnp.bfloat16)
    query_all = jnp.dot(latent_query, query_up, preferred_element_type=jnp.float32).reshape(
        tok_count, head_count, NOPE + ROPE
    )
    query_plain = query_all[:, :, :NOPE].astype(jnp.bfloat16)
    query_rope = rotate(query_all[:, :, NOPE:], angles_for(offsets, ROPE)[:, None, :]).astype(
        jnp.bfloat16
    )
    absorbed = jnp.einsum(
        "thd,rhd->htr",
        query_plain,
        key_up.reshape(KVR, head_count, NOPE),
        preferred_element_type=jnp.float32,
    ).astype(jnp.bfloat16)
    queries = jnp.concatenate([absorbed, jnp.transpose(query_rope, (1, 0, 2))], axis=-1)
    score_scale = (NOPE + ROPE) ** (-0.5)
    half_rows = tok_count // lax.axis_size("tp")
    first_row = lax.axis_index("tp") * half_rows
    own_rows = lax.dynamic_slice_in_dim(normed, first_row, half_rows, 0)
    own_positions = lax.dynamic_slice_in_dim(offsets, first_row, half_rows, 0)
    own_keys = key_block(own_rows, latent_down, latent_gain, rope_down, own_positions)
    block_keys = lax.all_gather(own_keys, ("sp", "tp"), axis=0, tiled=True)
    row_max = jnp.full((head_count, tok_count), far_below, jnp.float32)
    scores = (
        jnp.einsum("hqc,kc->hqk", queries, block_keys, preferred_element_type=jnp.float32)
        * score_scale
    )
    new_max = jnp.maximum(row_max, jnp.max(scores, axis=2))
    weights = jnp.exp(scores - new_max[:, :, None])
    new_sum = jnp.sum(weights, axis=2)
    added = jnp.einsum(
        "hqk,kr->hqr",
        weights.astype(jnp.bfloat16),
        block_keys[:, :KVR],
        preferred_element_type=jnp.float32,
    )
    gated_rows = (value_in * jax.nn.sigmoid(gate_in)).astype(jnp.bfloat16)
    padded = padded_2(gated_rows, (("sp", 0),), reach_rows)
    filtered = padded[0:tok_count].astype(jnp.float32) * conv_taps[0].astype(jnp.float32)
    for tap_index in range(1, conv_taps.shape[0]):
        filtered = filtered + padded[tap_index : tap_index + tok_count].astype(
            jnp.float32
        ) * conv_taps[tap_index].astype(jnp.float32)
    grouped = filtered.reshape(tok_count, -1, CH // GROUPS)
    centred = grouped - jnp.mean(grouped, axis=-1, keepdims=True)
    spread = jnp.mean(centred * centred, axis=-1, keepdims=True)
    normal_groups = (centred * lax.rsqrt(spread + norm_eps)).reshape(tok_count, -1)
    conv_branch = jax.nn.silu(normal_groups * group_gain.astype(jnp.float32)).astype(jnp.bfloat16)
    attended = (added / new_sum[:, :, None]).astype(jnp.bfloat16)
    log_weight = new_max + jnp.log(new_sum)
    head_out = jnp.einsum(
        "htr,rhv->thv",
        attended,
        value_up.reshape(KVR, head_count, VDIM),
        preferred_element_type=jnp.float32,
    )
    head_out = head_out.reshape(tok_count, head_count * VDIM).astype(jnp.bfloat16)
    mixed_in = jnp.concatenate([head_out, conv_branch], axis=1)
    out_weight = jnp.concatenate([head_proj, channel_proj], axis=0)
    partial_terms = jnp.dot(
        mixed_in,
        lax.all_gather(out_weight, "sp", axis=1, tiled=True),
        preferred_element_type=jnp.float32,
    )
    mixed_out = lax.psum_scatter(
        partial_terms.astype(jnp.bfloat16), "tp", scatter_dimension=1, tiled=True
    )
    return (mixed_out, log_weight)


LANES = 128
MESH = pl.DeviceIdType.MESH
F32 = jnp.float32
BF16 = jnp.bfloat16
Z_IN, X_IN, Y_IN, DX_IN, DY_IN = range(5)
Z_LOW, Z_HIGH, Z_FWD, X_OUT, Y_OUT, DX_OUT, DY_OUT = range(7)


def rope_tables(length):
    quarter = ROPE // 4
    inverse = np.float32(rope_base) ** (-np.arange(quarter, dtype=np.float32) / np.float32(quarter))
    positions = np.arange(length)
    row = (positions // GRID_W).astype(np.float32)[:, None] * inverse
    col = (positions % GRID_W).astype(np.float32)[:, None] * inverse
    angles = np.concatenate([row, col], axis=1).astype(np.float32)
    cosine, sine = np.cos(angles), np.sin(angles)
    tables = np.zeros((3, length, LANES), np.float32)
    half = ROPE // 2
    tables[0, :, :half] = cosine
    tables[0, :, half:ROPE] = cosine
    tables[1, :, :half] = -sine
    tables[2, :, half:ROPE] = sine
    return tables


def dot(a, b):
    return jnp.dot(a, b, preferred_element_type=F32)


def row_of(ref):
    return ref[...].reshape(1, -1)


def dot_nt(a, b):
    return lax.dot_general(a, b, (((1,), (1,)), ((), ())), preferred_element_type=F32)


def fused_kernel(
    n_sp,
    tokens, norm_gain, query_down, query_gain, latent_down, latent_gain, rope_down, query_up,
    key_up, value_up, glu_value, glu_gate, conv_taps, group_gain, head_proj, channel_proj, tables,
    out, log_out,
    w_q, w_v, w_t, w_o, tok_v, lat_v, rope_v, qup_v, kup_v, vup_v, tab_v,
    normed, keys, key_tmp, q_acc, q_lat, q_scr, v_acc, t_acc, mixed, gated, low_rows, high_rows, padded,
    parts, peer_parts,
    load_sem, recv_sem, send_sem, key_recv, key_send, key_pair_recv, key_pair_send, pair_recv, pair_send, halo_recv, halo_send,
):
    z = lax.axis_index("sp")
    c = lax.axis_index("fs")
    t = lax.axis_index("tp")
    peer = 1 - t
    c_x = c + 1 - 2 * (c % 2)
    c_y = (c + 2) % 4
    c_d = 3 - c
    rows = tokens.shape[0]
    depth = query_down.shape[0]
    q_cols = w_q.shape[2]
    chans = glu_value.shape[1]
    heads = key_up.shape[1] // NOPE
    head_rows = head_proj.shape[0]
    out_rows = w_o.shape[1]

    loads = {}

    def load(name, src, dst):
        copy = pltpu.make_async_copy(src, dst, load_sem.at[len(loads)])
        copy.start()
        loads[name] = copy

    load("wq", query_down.at[:, pl.ds(pl.multiple_of(t * q_cols, LANES), q_cols)], w_q.at[z])
    load("gv", glu_value, w_v.at[z])
    load("gg", glu_gate, w_t.at[z])
    load("tok", tokens, tok_v)
    load("lat", latent_down, lat_v)
    load("rope", rope_down, rope_v)
    load("tab", tables.at[:, pl.ds(pl.multiple_of(z * rows, LANES), rows), :], tab_v)
    load("hp", head_proj, w_o.at[z, pl.ds(0, head_rows), :])
    load("cp", channel_proj, w_o.at[z, pl.ds(head_rows, out_rows - head_rows), :])
    load("qup", query_up, qup_v)
    load("kup", key_up, kup_v)
    load("vup", value_up, vup_v)

    barrier = pltpu.get_barrier_semaphore()
    sides = [{"fs": c_x}, {"fs": c_y}, {"tp": peer}]
    for partner in sides:
        pl.semaphore_signal(barrier, inc=1, device_id=partner, device_id_type=MESH)

    @pl.when(z > 0)
    def _():
        pl.semaphore_signal(barrier, inc=1, device_id={"sp": z - 1}, device_id_type=MESH)

    @pl.when(z < n_sp - 1)
    def _():
        pl.semaphore_signal(barrier, inc=1, device_id={"sp": z + 1}, device_id_type=MESH)

    ends = (z == 0).astype(jnp.int32) + (z == n_sp - 1).astype(jnp.int32)
    pl.semaphore_wait(barrier, len(sides) + 2 - ends)

    direct_rows = (out_rows // 8) // 64 * 64
    units = [
        (w_q, 0, depth, True),
        (w_v, 0, depth, True),
        (w_t, 0, depth, True),
        (w_o, 0, head_rows, True),
        (w_o, head_rows, out_rows - head_rows - direct_rows, True),
        (w_o, out_rows - direct_rows, direct_rows, False),
    ]
    Q, V, T, H, P, D = range(6)

    def block(u, shard, quarter, half=None):
        buf, first, count, shared = units[u]
        if not shared:
            return buf.at[shard, pl.ds(first, count), :]
        size = count // 4
        start = first + quarter * size
        if half is not None:
            size = size // 2
            start = start + half * size
        return buf.at[shard, pl.ds(pl.multiple_of(start, 16), size), :]

    def remote(u, shard, ref, out_kind, in_kind, device):
        return pltpu.make_async_remote_copy(
            src_ref=ref, dst_ref=ref,
            send_sem=send_sem.at[u, shard, out_kind], recv_sem=recv_sem.at[u, shard, in_kind],
            device_id=device, device_id_type=MESH,
        )

    def own_copy(u, low):
        return remote(
            u, z, block(u, z, c), Z_LOW if low else Z_HIGH, Z_IN, {"sp": z - 1 if low else z + 1}
        )

    def send_own(u):
        @pl.when(z > 0)
        def _():
            own_copy(u, True).start()

        @pl.when(z < n_sp - 1)
        def _():
            own_copy(u, False).start()

    nearest = jnp.minimum(z, n_sp - 1 - z)
    arrivals = []
    for k in range(n_sp - 1):
        both = k < 2 * nearest
        distance = jnp.where(both, k // 2 + 1, k - nearest + 1)
        from_low = jnp.where(both, 1 - k % 2, (2 * z > n_sp - 1).astype(jnp.int32))
        shard = z - distance * (2 * from_low - 1)
        arrivals.append((shard, z + 2 * from_low - 1))

    def forward_copy(u, k):
        shard, target = arrivals[k]
        return remote(u, shard, block(u, shard, c), Z_FWD, Z_IN, {"sp": target})

    def when_forward(k, action):
        target = arrivals[k][1]

        @pl.when((target >= 0) & (target < n_sp))
        def _():
            action()

    def side_copies(u, k):
        shard, _ = arrivals[k]
        mine = block(u, shard, c)
        return (
            remote(u, shard, mine, X_OUT, X_IN, {"fs": c_x}),
            remote(u, shard, mine, Y_OUT, Y_IN, {"fs": c_y}),
        )

    def corner_copies(u, k):
        shard, _ = arrivals[k]
        return (
            remote(u, shard, block(u, shard, c_x, 0), DY_OUT, DY_IN, {"fs": c_y}),
            remote(u, shard, block(u, shard, c_y, 1), DX_OUT, DX_IN, {"fs": c_x}),
        )

    def wait_in(u, k, kind, quarter, half=None):
        shard, _ = arrivals[k]
        remote(u, shard, block(u, shard, quarter, half), Z_FWD, kind, {"fs": c_x}).wait_recv()

    def step_a(u, k):
        wait_in(u, k, Z_IN, c)
        when_forward(k, lambda: forward_copy(u, k).start())
        if units[u][3]:
            for copy in side_copies(u, k):
                copy.start()

    def step_b(u, k):
        to_y, to_x = corner_copies(u, k)
        wait_in(u, k, X_IN, c_x)
        to_y.start()
        wait_in(u, k, Y_IN, c_y)
        to_x.start()

    def step_c(u, k):
        wait_in(u, k, DY_IN, c_d, 0)
        wait_in(u, k, DX_IN, c_d, 1)

    for name, u in (("wq", Q), ("gv", V), ("gg", T)):
        loads[name].wait()
        send_own(u)

    loads["tok"].wait()
    values = tok_v[...].astype(F32)
    normed[...] = rms_scale(values, row_of(norm_gain)).astype(BF16)

    def rotate_lanes(v):
        half = ROPE // 2
        return (
            v * tab_v[0] + pltpu.roll(v, LANES - half, 1) * tab_v[1] + pltpu.roll(v, half, 1) * tab_v[2]
        )

    loads["lat"].wait()
    latent = rms_scale(dot(normed[...], lat_v[...]), row_of(latent_gain))
    keys[z, :, 0:KVR] = latent.astype(BF16)
    loads["rope"].wait()
    loads["tab"].wait()
    key_tmp[...] = jnp.zeros_like(key_tmp)
    key_tmp[:, 0:ROPE] = dot_nt(normed[...], rope_v[...])
    keys[z, :, KVR : KVR + LANES] = rotate_lanes(key_tmp[...]).astype(BF16)

    half_rows = rows // 2

    def key_half(shard, half):
        return keys.at[shard, pl.ds(pl.multiple_of(half * half_rows, 16), half_rows), :]

    def key_copy(shard, kind, target):
        return pltpu.make_async_remote_copy(
            src_ref=key_half(shard, t), dst_ref=key_half(shard, t),
            send_sem=key_send.at[shard, kind], recv_sem=key_recv.at[shard],
            device_id={"sp": target}, device_id_type=MESH,
        )

    def key_pair(shard, half):
        return pltpu.make_async_remote_copy(
            src_ref=key_half(shard, half), dst_ref=key_half(shard, half),
            send_sem=key_pair_send.at[shard], recv_sem=key_pair_recv.at[shard],
            device_id={"tp": peer}, device_id_type=MESH,
        )

    def own_keys(action):
        @pl.when(z > 0)
        def _():
            action(key_copy(z, Z_LOW, z - 1))

        @pl.when(z < n_sp - 1)
        def _():
            action(key_copy(z, Z_HIGH, z + 1))

    own_keys(lambda copy: copy.start())

    def step_k(k):
        shard, target = arrivals[k]
        key_copy(shard, Z_FWD, target).wait_recv()
        when_forward(k, lambda: key_copy(shard, Z_FWD, target).start())
        key_pair(shard, t).start()

    def add_shard(acc, weights, shard, first=False):
        columns = pl.ds(pl.multiple_of(shard * depth, LANES), depth)
        term = dot(normed[:, columns], weights[shard])
        acc[...] = term if first else acc[...] + term

    add_shard(q_acc, w_q, z, True)
    add_shard(v_acc, w_v, z, True)
    add_shard(t_acc, w_t, z, True)
    accs = {Q: (q_acc, w_q), V: (v_acc, w_v), T: (t_acc, w_t)}

    def step_cm(u, k):
        step_c(u, k)
        add_shard(*accs[u], arrivals[k][0])

    last = n_sp - 2
    loads["hp"].wait()
    loads["cp"].wait()
    for k in range(last + 1):
        for u in (Q, V, T):
            step_a(u, k)
            if k:
                step_b(u, k - 1)
            if k > 1:
                step_cm(u, k - 2)
        step_k(k)
        if k == 1:
            send_own(H)
    send_own(P)
    step_b(Q, last)
    step_a(H, 0)
    step_b(V, last)
    step_a(H, 1)
    step_b(T, last)
    send_own(D)
    for u in (Q, V, T):
        step_cm(u, last - 1)
    step_b(H, 0)
    step_a(P, 0)
    step_cm(Q, last)
    step_a(H, 2)

    q_lat[t] = q_acc[...]
    q_copy = pltpu.make_async_remote_copy(
        src_ref=q_lat.at[t], dst_ref=q_lat.at[t], send_sem=pair_send.at[0], recv_sem=pair_recv.at[0],
        device_id={"tp": peer}, device_id_type=MESH,
    )
    q_copy.start()
    loads["qup"].wait()
    loads["kup"].wait()
    loads["vup"].wait()
    pltpu.make_async_remote_copy(
        src_ref=q_lat.at[peer], dst_ref=q_lat.at[peer], send_sem=pair_send.at[0],
        recv_sem=pair_recv.at[0], device_id={"tp": peer}, device_id_type=MESH,
    ).wait_recv()
    whole_q = jnp.concatenate([q_lat[0], q_lat[1]], axis=1)
    latent_query = rms_scale(whole_q, row_of(query_gain)).astype(BF16)
    q_scr[...] = dot(latent_query, qup_v[...])
    for k in range(n_sp - 1):
        key_pair(arrivals[k][0], peer).wait_recv()

    def attend(h, shifted):
        start = h * (NOPE + ROPE)
        source = q_scr[...]
        if start % LANES:
            source, start = shifted, start - ROPE
        plain = source[:, start : start + NOPE].astype(BF16)
        rope_part = rotate_lanes(source[:, start + NOPE : start + NOPE + LANES]).astype(BF16)
        absorbed = dot_nt(plain, kup_v[:, h * NOPE : (h + 1) * NOPE]).astype(BF16)
        query = jnp.concatenate([absorbed, rope_part], axis=1)
        all_keys = keys[...].reshape(n_sp * rows, KVR + LANES)
        scores = dot_nt(query, all_keys) * (NOPE + ROPE) ** (-0.5)
        row_max = jnp.max(scores, axis=1, keepdims=True)
        weights = jnp.exp(scores - row_max)
        total = jnp.sum(weights, axis=1, keepdims=True)
        added = dot(weights.astype(BF16), all_keys[:, 0:KVR])
        attended = (added / total).astype(BF16)
        head_out = dot(attended, vup_v[:, h * VDIM : (h + 1) * VDIM])
        mixed[:, h * VDIM : (h + 1) * VDIM] = head_out.astype(BF16)
        return row_max + jnp.log(total)

    whole = q_scr[...]
    shifted = pltpu.roll(whole, whole.shape[1] - ROPE, 1)
    lane = lax.broadcasted_iota(jnp.int32, (rows, LANES), 1)
    logs = jnp.zeros((rows, LANES), F32)
    relays = [
        lambda: step_a(P, 1), lambda: step_b(H, 1), lambda: (step_a(D, 0), step_a(P, 2)),
        lambda: step_b(P, 0),
    ]
    for h in range(heads):
        logs = jnp.where(lane == h, attend(h, shifted), logs)
        relays[h]()
    log_out[...] = jnp.transpose(logs)[0:heads, :]

    step_cm(V, last)
    step_cm(T, last)

    halo = low_rows.shape[0]
    reach = conv_taps.shape[0] // 2
    gated[...] = (v_acc[...] * jax.nn.sigmoid(t_acc[...])).astype(BF16)
    up_copy = pltpu.make_async_remote_copy(
        src_ref=gated.at[pl.ds(rows - halo, halo), :], dst_ref=low_rows,
        send_sem=halo_send.at[0], recv_sem=halo_recv.at[0],
        device_id={"sp": z + 1}, device_id_type=MESH,
    )
    down_copy = pltpu.make_async_remote_copy(
        src_ref=gated.at[pl.ds(0, halo), :], dst_ref=high_rows,
        send_sem=halo_send.at[1], recv_sem=halo_recv.at[1],
        device_id={"sp": z - 1}, device_id_type=MESH,
    )

    @pl.when(z < n_sp - 1)
    def _():
        up_copy.start()

    @pl.when(z > 0)
    def _():
        down_copy.start()

    padded[halo : halo + rows, :] = gated[...].astype(F32)
    step_a(D, 1)
    step_b(H, 2)

    @pl.when(z > 0)
    def _():
        up_copy.wait_recv()
        padded[0:halo, :] = low_rows[...].astype(F32)

    @pl.when(z == 0)
    def _():
        padded[0:halo, :] = jnp.zeros((halo, chans), F32)

    @pl.when(z < n_sp - 1)
    def _():
        down_copy.wait_recv()
        padded[halo + rows : 2 * halo + rows, :] = high_rows[...].astype(F32)

    @pl.when(z == n_sp - 1)
    def _():
        padded[halo + rows : 2 * halo + rows, :] = jnp.zeros((halo, chans), F32)

    group = CH // GROUPS
    gains = row_of(group_gain).astype(F32)
    between = [
        lambda: step_b(P, 1), lambda: step_c(H, 0), lambda: step_a(D, 2), lambda: step_b(P, 2),
    ]
    for g in range(chans // group):
        lanes = slice(g * group, (g + 1) * group)
        taps = conv_taps[:, lanes].astype(F32)
        filtered = jnp.zeros((rows, group), F32)
        for j in range(conv_taps.shape[0]):
            first = halo - reach + j
            filtered = filtered + padded[first : first + rows, lanes] * taps[j : j + 1, :]
        centred = filtered - jnp.mean(filtered, axis=1, keepdims=True)
        spread = jnp.mean(centred * centred, axis=1, keepdims=True)
        branch = centred * lax.rsqrt(spread + norm_eps) * gains[:, lanes]
        branch = branch * jax.nn.sigmoid(branch)
        mixed[:, heads * VDIM + g * group : heads * VDIM + (g + 1) * group] = branch.astype(BF16)
        between[g]()

    half_sp = n_sp // 2

    def p_copy(i):
        return pltpu.make_async_remote_copy(
            src_ref=parts.at[peer * half_sp + i], dst_ref=peer_parts.at[i],
            send_sem=pair_send.at[1 + i], recv_sem=pair_recv.at[1 + i],
            device_id={"tp": peer}, device_id_type=MESH,
        )

    def add_part(shard, between_halves):
        part = dot(mixed[:, 0:head_rows], w_o[shard, 0:head_rows, :])
        between_halves()
        part = part + dot(mixed[:, head_rows:out_rows], w_o[shard, head_rows:out_rows, :])
        parts[shard] = part.astype(BF16)
        for i in range(half_sp):
            @pl.when(shard == peer * half_sp + i)
            def _():
                p_copy(i).start()

    add_part(z, lambda: None)
    for k in range(n_sp - 1):
        if k:
            step_c(H, k)
        add_part(arrivals[k][0], functools.partial(step_c, P, k))

    for u in range(len(units)):
        @pl.when(z > 0)
        def _():
            own_copy(u, True).wait_send()

        @pl.when(z < n_sp - 1)
        def _():
            own_copy(u, False).wait_send()

        for k in range(n_sp - 1):
            when_forward(k, lambda: forward_copy(u, k).wait_send())
            if units[u][3]:
                for copy in side_copies(u, k) + corner_copies(u, k):
                    copy.wait_send()
    own_keys(lambda copy: copy.wait_send())
    for k in range(n_sp - 1):
        shard, target = arrivals[k]
        when_forward(k, lambda: key_copy(shard, Z_FWD, target).wait_send())
        key_pair(shard, t).wait_send()
    q_copy.wait_send()

    @pl.when(z < n_sp - 1)
    def _():
        up_copy.wait_send()

    @pl.when(z > 0)
    def _():
        down_copy.wait_send()

    for i in range(half_sp):
        p_copy(i).wait()
    width = parts.shape[2]
    for i in range(half_sp):
        total = parts[t * half_sp + i].astype(F32) + peer_parts[i].astype(F32)
        out[:, i * width : (i + 1) * width] = total.astype(BF16)


def fused_device(n_sp, *args):
    (tokens, norm_gain, query_down, query_gain, latent_down, latent_gain, rope_down, query_up,
     key_up, value_up, glu_value, glu_gate, conv_taps, group_gain, head_proj, channel_proj) = args
    rows, width = tokens.shape
    depth, q_rank = query_down.shape
    chans = glu_value.shape[1]
    heads = key_up.shape[1] // NOPE
    out_rows = head_proj.shape[0] + channel_proj.shape[0]
    cols = head_proj.shape[1]
    halo = (conv_taps.shape[0] // 2 + 15) // 16 * 16
    tables = jnp.asarray(rope_tables(n_sp * rows))
    vmem = pl.BlockSpec(memory_space=pltpu.VMEM)
    hbm = pl.BlockSpec(memory_space=pltpu.HBM)
    as_row = lambda v: v
    operands = [
        (tokens, hbm), (as_row(norm_gain), vmem), (query_down, hbm), (as_row(query_gain), vmem),
        (latent_down, hbm), (as_row(latent_gain), vmem), (rope_down.T, hbm), (query_up, hbm),
        (key_up, hbm), (value_up, hbm), (glu_value, hbm), (glu_gate, hbm), (conv_taps, vmem),
        (as_row(group_gain), vmem), (head_proj, hbm), (channel_proj, hbm), (tables, hbm),
    ]
    like = lambda a: pltpu.VMEM(a.shape, a.dtype)
    dma = pltpu.SemaphoreType.DMA
    scratch = [
        pltpu.VMEM((n_sp, depth, q_rank // 2), BF16),
        pltpu.VMEM((n_sp, depth, chans), BF16),
        pltpu.VMEM((n_sp, depth, chans), BF16),
        pltpu.VMEM((n_sp, out_rows, cols), BF16),
        like(tokens), like(latent_down), pltpu.VMEM(rope_down.shape[::-1], BF16), like(query_up), like(key_up), like(value_up),
        pltpu.VMEM((3, rows, LANES), F32),
        pltpu.VMEM((rows, width), BF16),
        pltpu.VMEM((n_sp, rows, KVR + LANES), BF16),
        pltpu.VMEM((rows, LANES), F32),
        pltpu.VMEM((rows, q_rank // 2), F32),
        pltpu.VMEM((2, rows, q_rank // 2), F32),
        pltpu.VMEM((rows, query_up.shape[1]), F32),
        pltpu.VMEM((rows, chans), F32),
        pltpu.VMEM((rows, chans), F32),
        pltpu.VMEM((rows, out_rows), BF16),
        pltpu.VMEM((rows, chans), BF16),
        pltpu.VMEM((halo, chans), BF16),
        pltpu.VMEM((halo, chans), BF16),
        pltpu.VMEM((rows + 2 * halo, chans), F32),
        pltpu.VMEM((n_sp, rows, cols), BF16),
        pltpu.VMEM((n_sp // 2, rows, cols), BF16),
        dma((12,)), dma((6, n_sp, 5)), dma((6, n_sp, 7)), dma((n_sp,)), dma((n_sp, 3)), dma((n_sp,)),
        dma((n_sp,)),
        dma((1 + n_sp // 2,)), dma((1 + n_sp // 2,)), dma((2,)), dma((2,)),
    ]
    return pl.pallas_call(
        functools.partial(fused_kernel, n_sp),
        out_shape=(
            jax.ShapeDtypeStruct((rows, n_sp * cols // 2), BF16),
            jax.ShapeDtypeStruct((heads, rows), F32),
        ),
        in_specs=[spec for _, spec in operands],
        out_specs=(vmem, vmem),
        scratch_shapes=scratch,
        compiler_params=pltpu.CompilerParams(
            collective_id=0, has_side_effects=True, vmem_limit_bytes=63 * 1024 * 1024
        ),
        name="fused_layer",
    )(*[value for value, _ in operands])


def solution(mesh):
    in_specs = (
        P(("fs", "sp"), None),
        P(),
        P("sp", None),
        P(),
        P(),
        P(),
        P(),
        P(None, "tp"),
        P(None, "tp"),
        P(None, "tp"),
        P("sp", "tp"),
        P("sp", "tp"),
        P(None, "tp"),
        P("tp"),
        P("tp", "sp"),
        P("tp", "sp"),
    )
    out_specs = (P(("fs", "sp"), "tp"), P("tp", ("fs", "sp")))
    body = per_device
    if mesh.shape["fs"] == 4 and mesh.shape["tp"] == 2 and mesh.shape["sp"] == 4:
        body = functools.partial(fused_device, mesh.shape["sp"])
    return jax.shard_map(
        body, mesh=mesh, in_specs=in_specs, out_specs=out_specs, check_vma=False
    )
```
